32 devices in a mesh: sp: 4 (over z), fs: 4 (over y, x), tp: 2 (over core).
Axes of the slice: x: 2, y: 2, z: 4, core: 2. Of those that a mesh axis runs over, the one named last changes fastest.
Arguments:
- tokens: bfloat16 [4, 4096, 2048], P('fs', ('sp', 'tp')), may hold values from -6 to 6
- norm_gain: bfloat16 [2048], replicated, may hold values from 0.099609375 to 1.8984375
- w_query: bfloat16 [2048, 1024], P(None, 'tp'), may hold values from -0.125 to 0.125
- w_key: bfloat16 [2048, 1024], P(None, 'tp'), may hold values from -0.125 to 0.125
- w_value: bfloat16 [2048, 1024], P(None, 'tp'), may hold values from -0.125 to 0.125
- w_outgate: bfloat16 [2048, 1024], P(None, 'tp'), may hold values from -0.125 to 0.125
- w_gatein: bfloat16 [2048, 1024], P(None, 'tp'), may hold values from -0.125 to 0.125
- w_gateout: bfloat16 [2048, 1024], P(None, 'tp'), may hold values from -0.125 to 0.125
- w_convin: bfloat16 [2048, 1024], P(None, 'tp'), may hold values from -0.125 to 0.125
- w_igate: bfloat16 [2048, 8], replicated, may hold values from -0.125 to 0.125
- w_fgate: bfloat16 [2048, 8], replicated, may hold values from -0.125 to 0.125
- input_bias: float32 [8], replicated, may hold values from -1 to 101
- forget_bias: float32 [8], replicated
- forget_extra: float32 [4, 4096, 8], P('fs', 'sp', 'tp'), may hold values from -0.7 to 0
- init_memory: float32 [4, 8, 128, 128], P('fs', 'tp'), may hold values from -56 to 56
- head_gain: bfloat16 [1024], replicated, may hold values from 0.099609375 to 1.8984375
- conv_taps: bfloat16 [3, 1024], replicated, may hold values from -3.5 to 3.5
- out_memory: bfloat16 [1024, 2048], P('tp'), may hold values from -0.125 to 0.125
- out_conv: bfloat16 [1024, 2048], P('tp'), may hold values from -0.125 to 0.125
Outputs:
- layer_out: bfloat16 [4, 4096, 2048], P('fs', ('sp', 'tp'))
The draws below stay inside these ranges and needn't reach their ends.
All inputs are finite; a program needn't handle non-finite values.
Results may differ from the reference program's by a relative error of at most 0.017.
Values may be sent and summed in bfloat16 or wider, within the bound.
A program may use at most 128 MiB of HBM per device.

```python
import math
import jax
import jax.numpy as jnp
from jax import lax

D = 2048
MEMORY_HEADS = 8
DH = 128
HALF = 1024
BLOCK = 128
TAPS = 3
TOK_DEV = 1024
SEQUENCE_COUNT = 4
SEQUENCE_LENGTH = 4096
N_TP = 2


def draw_input_bias(key, part):
    base_key = jax.random.fold_in(jax.random.fold_in(key, 11), 0)
    steady_forget = jax.random.uniform(base_key, (MEMORY_HEADS,), jnp.float32, -1.0, 1.0)
    return steady_forget


def draw_forget_bias(key, part):
    slow_key, fast_key, pick_key = jax.random.split(jax.random.fold_in(key, 23), 3)
    slow_bias = math.log(SEQUENCE_LENGTH) + jax.random.uniform(slow_key, (MEMORY_HEADS,), jnp.float32, 1.5, 3.0)
    fast_bias = jax.random.uniform(fast_key, (MEMORY_HEADS,), jnp.float32, 3.4, 4.6)
    chosen = jax.random.permutation(pick_key, MEMORY_HEADS) < MEMORY_HEADS // 2
    return jnp.where(chosen, fast_bias, slow_bias)


def draw_forget_extra(key, part):
    rate_key, place_random_key, drop_random_key = jax.random.split(jax.random.fold_in(key, 37), 3)
    span_count = SEQUENCE_LENGTH // TOK_DEV
    span_rates = jnp.exp(jax.random.uniform(rate_key, (SEQUENCE_COUNT, span_count, 1, MEMORY_HEADS), jnp.float32, math.log(0.1), math.log(0.8))) / SEQUENCE_LENGTH
    steady_forget = -jnp.broadcast_to(span_rates, (SEQUENCE_COUNT, span_count, TOK_DEV, MEMORY_HEADS)).reshape(SEQUENCE_COUNT, SEQUENCE_LENGTH, MEMORY_HEADS)
    sudden_drop_places = jax.random.randint(place_random_key, (SEQUENCE_COUNT, 2), 0, SEQUENCE_LENGTH)
    sudden_drop_mask = jnp.any(jnp.arange(SEQUENCE_LENGTH)[None, :, None] == sudden_drop_places[:, None, :], axis=-1)
    sudden_drop_values = jax.random.uniform(drop_random_key, (SEQUENCE_COUNT, SEQUENCE_LENGTH, MEMORY_HEADS), jnp.float32, math.log(0.5), math.log(0.8))
    return steady_forget + jnp.where(sudden_drop_mask[:, :, None], sudden_drop_values, 0.0)


def shard_levels(key, extent, cuts, smallest, top_value):
    level = 1.0
    for dim, parts in cuts:
        steps = jax.random.uniform(jax.random.fold_in(jax.random.fold_in(key, 6), dim), (parts,), jnp.float32, smallest / len(cuts), top_value / len(cuts))
        level = level * jnp.repeat(jnp.exp(steps), extent[dim] // parts).reshape((-1,) + (1,) * (len(extent) - 1 - dim))
    return level


def gaussian(own_key, extent, spread, reach, shards=(), held_as=jnp.bfloat16):
    result = spread * jax.random.normal(own_key, extent, jnp.float32)
    if shards:
        result = result * shard_levels(own_key, extent, shards, -0.22, 0.18)
    return jnp.clip(result, -reach, reach).astype(held_as)


def setup_inputs(seed: int = 0) -> dict:
    seeds = jax.random.split(jax.random.key(seed), 20)
    return {
        "tokens": gaussian(seeds[0], (SEQUENCE_COUNT, SEQUENCE_LENGTH, D), 1.0, 6.0, ((0, 4), (1, 8))),
        "norm_gain": jnp.clip(1.0 + 0.18 * jax.random.normal(seeds[1], (D,), jnp.float32), 0.099609375, 1.8984375).astype(jnp.bfloat16),
        "w_query": gaussian(seeds[2], (D, HALF), D ** -0.5, 0.125, ((1, 2),)),
        "w_key": gaussian(seeds[3], (D, HALF), D ** -0.5, 0.125, ((1, 2),)),
        "w_value": gaussian(seeds[4], (D, HALF), D ** -0.5, 0.125, ((1, 2),)),
        "w_outgate": gaussian(seeds[5], (D, HALF), D ** -0.5, 0.125, ((1, 2),)),
        "w_gatein": gaussian(seeds[6], (D, HALF), D ** -0.5, 0.125, ((1, 2),)),
        "w_gateout": gaussian(seeds[7], (D, HALF), D ** -0.5, 0.125, ((1, 2),)),
        "w_convin": gaussian(seeds[8], (D, HALF), D ** -0.5, 0.125, ((1, 2),)),
        "w_igate": gaussian(seeds[9], (D, MEMORY_HEADS), D ** -0.5, 0.125),
        "w_fgate": gaussian(seeds[10], (D, MEMORY_HEADS), D ** -0.5, 0.125),
        "input_bias": draw_input_bias(jax.random.fold_in(seeds[19], 71), 0),
        "forget_bias": draw_forget_bias(jax.random.fold_in(seeds[19], 71), 0),
        "forget_extra": draw_forget_extra(jax.random.fold_in(seeds[19], 71), 0),
        "init_memory": gaussian(seeds[14], (SEQUENCE_COUNT, MEMORY_HEADS, DH, DH), (0.15 * SEQUENCE_LENGTH ** 0.5), 56.0, ((0, 4), (1, 2)), jnp.float32),
        "head_gain": jnp.clip(1.0 + 0.18 * jax.random.normal(seeds[15], (HALF,), jnp.float32), 0.099609375, 1.8984375).astype(jnp.bfloat16),
        "conv_taps": gaussian(seeds[16], (TAPS, HALF), TAPS ** -0.5, 3.5),
        "out_memory": gaussian(seeds[17], (HALF, D), (2 * HALF) ** -0.5, 0.125, ((0, 2),)),
        "out_conv": gaussian(seeds[18], (HALF, D), (2 * HALF) ** -0.5, 0.125, ((0, 2),)),
    }


EPSILON = 1e-06

def memory_cell(queries, key_rows, value_rows, input_pre, log_forget, start_memory):
    nblocks = SEQUENCE_LENGTH // BLOCK
    key_factor = DH ** (-0.5)
    highest = lax.Precision.HIGHEST

    def blocked(matrix):
        return jnp.swapaxes(matrix.reshape(nblocks, BLOCK, MEMORY_HEADS, DH), 1, 2).astype(jnp.float32)

    def gate_blocks(matrix):
        return jnp.swapaxes(matrix.reshape(nblocks, BLOCK, MEMORY_HEADS), 1, 2)
    causal = jnp.tril(jnp.ones((BLOCK, BLOCK), dtype=bool))

    def advance(memory_pair, inputs):
        memory, log_scale = memory_pair
        query_blk, key_blk, value_blk, gate_in_blk, forget_blk = inputs
        cumulative = jnp.cumsum(forget_blk, axis=-1)
        block_total = cumulative[:, -1]
        exponent = block_total[:, None] - cumulative + gate_in_blk
        block_top = lax.optimization_barrier(jnp.max(exponent, axis=-1))
        weighted_keys = (jnp.exp(exponent - block_top[:, None])[:, :, None] * key_blk * key_factor).astype(jnp.bfloat16)
        weighted_keys = lax.optimization_barrier(weighted_keys).astype(jnp.float32)
        block_terms = jnp.einsum('hsd,hse->hde', weighted_keys, value_blk, precision=highest)
        pair_log = cumulative[:, :, None] - cumulative[:, None, :] + gate_in_blk[:, None, :]
        pair_log = jnp.where(causal, pair_log, -jnp.inf)
        carried_log = cumulative + log_scale[:, None]
        row_top = jnp.maximum(carried_log, lax.optimization_barrier(jnp.max(pair_log, axis=-1)))
        scores = jnp.einsum('htd,hsd->hts', query_blk, key_blk, precision=highest) * key_factor
        weighted = (jnp.exp(pair_log - row_top[:, :, None]) * scores).astype(jnp.bfloat16)
        weighted = lax.optimization_barrier(weighted).astype(jnp.float32)
        carried = jnp.einsum('htd,hde->hte', query_blk, memory, precision=highest)
        readout = jnp.exp(carried_log - row_top)[:, :, None] * carried
        readout = readout + jnp.einsum('hts,hse->hte', weighted, value_blk, precision=highest)
        new_scale = jnp.maximum(block_total + log_scale, block_top)
        new_memory = jnp.exp(block_total + log_scale - new_scale)[:, None, None] * memory
        new_memory = new_memory + jnp.exp(block_top - new_scale)[:, None, None] * block_terms
        return ((new_memory, new_scale), readout)
    start_pair = (start_memory, jnp.zeros((MEMORY_HEADS,), jnp.float32))
    inputs = (blocked(queries), blocked(key_rows), blocked(value_rows), gate_blocks(input_pre), gate_blocks(log_forget))
    final_pair, readouts = lax.scan(advance, start_pair, inputs)
    return jnp.swapaxes(readouts, 1, 2).reshape(SEQUENCE_LENGTH, HALF)

def reference(tokens, norm_gain, w_query, w_key, w_value, w_outgate, w_gatein, w_gateout, w_convin, w_igate, w_fgate, input_bias, forget_bias, forget_extra, init_memory, head_gain, conv_taps, out_memory, out_conv):
    group_width = HALF // N_TP
    outputs = []
    for seq_index in range(SEQUENCE_COUNT):
        seq_rows = tokens[seq_index].astype(jnp.float32)
        normed = seq_rows * lax.rsqrt(lax.optimization_barrier(jnp.mean(seq_rows * seq_rows, axis=-1, keepdims=True)) + EPSILON)
        normed = (normed * norm_gain.astype(jnp.float32)).astype(jnp.bfloat16)

        def project(weight):
            return jnp.dot(normed, weight, preferred_element_type=jnp.float32).astype(jnp.bfloat16)
        queries = project(w_query)
        key_rows = project(w_key)
        value_rows = project(w_value)
        out_gate = project(w_outgate)
        gate_in = project(w_gatein)
        gate_out = project(w_gateout)
        conv_input = project(w_convin)
        input_pre = jnp.dot(normed, w_igate, preferred_element_type=jnp.float32) + input_bias
        forget_pre = jnp.dot(normed, w_fgate, preferred_element_type=jnp.float32) + forget_bias
        log_forget = jax.nn.log_sigmoid(forget_pre) + forget_extra[seq_index]
        readout = memory_cell(queries, key_rows, value_rows, input_pre, log_forget, init_memory[seq_index])
        per_head = readout.reshape(SEQUENCE_LENGTH, MEMORY_HEADS, DH)
        normalized = per_head * lax.rsqrt(lax.optimization_barrier(jnp.mean(per_head * per_head, axis=-1, keepdims=True)) + EPSILON)
        memory_out = normalized.reshape(SEQUENCE_LENGTH, HALF) * head_gain.astype(jnp.float32) * jax.nn.sigmoid(out_gate.astype(jnp.float32))
        memory_out = memory_out.astype(jnp.bfloat16)
        conv_product = (gate_in.astype(jnp.float32) * conv_input.astype(jnp.float32)).astype(jnp.bfloat16)
        conv_product = lax.optimization_barrier(conv_product).astype(jnp.float32)
        padded = jnp.pad(conv_product, ((TAPS - 1, 0), (0, 0)))
        mixed_conv = jnp.zeros((SEQUENCE_LENGTH, HALF), jnp.float32)
        for tap_index in range(TAPS):
            mixed_conv = mixed_conv + padded[tap_index:tap_index + SEQUENCE_LENGTH] * conv_taps[tap_index].astype(jnp.float32)
        conv_out = (gate_out.astype(jnp.float32) * mixed_conv).astype(jnp.bfloat16)
        summed = jnp.zeros((SEQUENCE_LENGTH, D), jnp.float32)
        for part_index in range(N_TP):
            low_col = part_index * group_width
            high_col = low_col + group_width
            partial_value = jnp.dot(memory_out[:, low_col:high_col], out_memory[low_col:high_col], preferred_element_type=jnp.float32)
            partial_value = partial_value + jnp.dot(conv_out[:, low_col:high_col], out_conv[low_col:high_col], preferred_element_type=jnp.float32)
            summed = summed + lax.optimization_barrier(partial_value.astype(jnp.bfloat16)).astype(jnp.float32)
        outputs.append(summed.astype(jnp.bfloat16))
    return jnp.stack(outputs)
```

```python
import functools

import jax
import jax.numpy as jnp
from jax import lax
from jax.experimental import pallas as pl
from jax.experimental.pallas import tpu as pltpu
from jax.sharding import PartitionSpec as P

BLOCK = 128
EPSILON = 1e-06
LOWEST_LOG = -1e30
MESH = pl.DeviceIdType.MESH
F32 = jnp.float32
BF16 = jnp.bfloat16
PAD = 8
RIM = 16
NORM_ROWS = 64
BATCHES = 2

KEY, VALUE, QUERY, GATE_IN, CONV_IN, GATE_OUT, OUT_GATE = range(7)


def kernel(
    n_sp,
    tokens,
    norm_gain,
    w_key,
    w_value,
    w_query,
    w_gatein,
    w_convin,
    w_gateout,
    w_outgate,
    w_igate,
    w_fgate,
    input_bias,
    forget_bias,
    extra_in,
    init_in,
    head_gain,
    taps_in,
    out_memory,
    out_conv,
    layer_out,
    tok,
    gain_in,
    gain_row,
    head_in,
    head_rows,
    igate_in,
    fgate_in,
    gate_w,
    bias_in,
    extra,
    init_memory,
    conv_taps,
    normed,
    weights,
    out_m,
    out_c,
    k_rows,
    v_rows,
    q_rows,
    conv_pair,
    go_rows,
    og_rows,
    gate_pre,
    row_log,
    col_log,
    block_sum,
    block_peak,
    prefix,
    prefix_cols,
    half_sum,
    half_log,
    half_total,
    relay_rows,
    carry,
    carry_log,
    carry_cols,
    send_memory,
    send_log,
    local_out,
    local_top,
    conv_rows,
    rim,
    rim_out,
    mix_conv,
    mix_memory,
    acc,
    token_sem,
    small_sem,
    weight_sem,
    norm_send,
    norm_recv,
    outw_send,
    outw_recv,
    state_send,
    state_recv,
    rim_sem,
    conv_sem,
    mem_send,
    mem_recv,
):
    me = lax.axis_index("tp")
    other = 1 - me
    place = lax.axis_index("sp")
    half = tok.shape[0]
    total_rows = normed.shape[0]
    width = k_rows.shape[1]
    heads = init_memory.shape[0]
    dh = init_memory.shape[1]
    n_half = half // BLOCK
    nblocks = total_rows // BLOCK
    key_factor = dh ** (-0.5)
    out_width = layer_out.shape[1]
    n_out = n_half
    out_cols = out_width // n_out
    group = heads // BATCHES

    barrier = pltpu.get_barrier_semaphore()
    pl.semaphore_signal(barrier, inc=1, device_id={"tp": other}, device_id_type=MESH)

    @pl.when(place > 0)
    def _():
        pl.semaphore_signal(barrier, inc=1, device_id={"sp": place - 1}, device_id_type=MESH)

    def rows_of(index, size):
        return pl.ds(pl.multiple_of(index * size, size), size)

    tok_copies = [
        pltpu.make_async_copy(
            tokens.at[pl.ds(c * BLOCK, BLOCK)], tok.at[pl.ds(c * BLOCK, BLOCK)], token_sem.at[c]
        )
        for c in range(n_half)
    ]
    smalls = [
        pltpu.make_async_copy(src, dst, small_sem.at[i])
        for i, (src, dst) in enumerate(
            (
                (norm_gain, gain_in),
                (w_igate, igate_in),
                (w_fgate, fgate_in),
                (input_bias, bias_in.at[0]),
                (forget_bias, bias_in.at[1]),
                (extra_in, extra),
                (init_in, init_memory),
                (head_gain, head_in),
                (taps_in, conv_taps),
            )
        )
    ]
    w_in = (w_key, w_value, w_query, w_gatein, w_convin, w_gateout, w_outgate)
    w_copies = [
        pltpu.make_async_copy(w, weights.at[s], weight_sem.at[s]) for s, w in enumerate(w_in)
    ]
    out_copies = [
        pltpu.make_async_copy(out_memory, out_m.at[pl.ds(0, width)], weight_sem.at[7]),
        pltpu.make_async_copy(out_conv, out_c.at[pl.ds(0, width)], weight_sem.at[8]),
    ]

    def partner_copy(src, dst, send_sem, recv_sem):
        return pltpu.make_async_remote_copy(
            src_ref=src,
            dst_ref=dst,
            send_sem=send_sem,
            recv_sem=recv_sem,
            device_id={"tp": other},
            device_id_type=MESH,
        )

    def norm_copy(c):
        rows = pl.ds(pl.multiple_of(me * half + c * BLOCK, BLOCK), BLOCK)
        return partner_copy(normed.at[rows], normed.at[rows], norm_send.at[c], norm_recv.at[c])

    outw_copies = [
        partner_copy(src, dst.at[pl.ds(width, width)], outw_send.at[i], outw_recv.at[i])
        for i, (src, dst) in enumerate(((out_conv, out_c), (out_memory, out_m)))
    ]

    smalls[0].start()
    for c in tok_copies:
        c.start()
    for c in smalls[1:]:
        c.start()

    smalls[0].wait()
    for j in range(norm_gain.shape[0]):
        gain_row[:, j * BLOCK : (j + 1) * BLOCK] = gain_in[j : j + 1].astype(F32)

    def normalize(c):
        @pl.loop(0, BLOCK // NORM_ROWS)
        def _(part):
            start = c * BLOCK + part * NORM_ROWS
            x = tok[pl.ds(pl.multiple_of(start, NORM_ROWS), NORM_ROWS), :].astype(F32)
            scale = lax.rsqrt(jnp.mean(x * x, axis=-1, keepdims=True) + EPSILON)
            y = (x * scale) * gain_row[...]
            normed[pl.ds(pl.multiple_of(me * half + start, NORM_ROWS), NORM_ROWS), :] = y.astype(
                BF16
            )

    first_weights = 3
    smalls[1].wait()
    smalls[2].wait()
    gates = jnp.concatenate(
        [
            fgate_in[...],
            igate_in[...],
            jnp.zeros((BLOCK - 2 * PAD, igate_in.shape[1]), BF16),
        ],
        axis=0,
    )
    gate_w[...] = jnp.transpose(gates)
    for c in range(n_half):
        tok_copies[c].wait()
        if c < first_weights:
            w_copies[c].start()
        normalize(c)
    for c in w_copies[min(first_weights, n_half) :]:
        c.start()

    for c in smalls[3:]:
        c.wait()
    head_rows[...] = head_in[...].astype(F32)

    @pl.when(place == 0)
    def _():
        for h in range(heads):
            carry[0, h] = init_memory[h].astype(BF16)
        carry_log[0] = jnp.zeros((PAD, BLOCK), F32)

    row_i = lax.broadcasted_iota(jnp.int32, (BLOCK, BLOCK), 0)
    col_i = lax.broadcasted_iota(jnp.int32, (BLOCK, BLOCK), 1)
    upper = jnp.where(row_i <= col_i, 1.0, 0.0).astype(F32)
    causal = col_i <= row_i

    def head_cols(h):
        return slice(h * dh, (h + 1) * dh)

    first_head = me * heads
    to_front = lax.rem(PAD - first_head, PAD)
    lane_head = lax.broadcasted_iota(jnp.int32, (PAD, BLOCK), 0)
    bias_f = jnp.zeros((PAD, BLOCK), F32)
    bias_i = jnp.zeros((PAD, BLOCK), F32)
    for h in range(heads):
        bias_i = jnp.where(lane_head == h, bias_in[0, first_head + h], bias_i)
        bias_f = jnp.where(lane_head == h, bias_in[1, first_head + h], bias_f)
    no_head = jnp.zeros((PAD - heads, BLOCK), F32)

    def dot(a, b):
        return jnp.dot(a, b, preferred_element_type=F32)

    def project(target, slot, rows):
        target[rows, :] = dot(normed[rows, :], weights[slot]).astype(BF16)

    def gate_math(index):
        forget_rows, in_rows = [], []
        for j in range(n_half):
            span = rows_of(index * n_half + j, BLOCK)
            pre = jnp.transpose(gate_pre[span, :])
            v = pltpu.roll(pre[0:PAD], to_front, 0) + bias_f
            log_forget = jnp.minimum(v, 0.0) - jnp.log1p(jnp.exp(-jnp.abs(v)))
            forget_rows.append(log_forget + jnp.concatenate([extra[:, span], no_head], axis=0))
            in_rows.append(pltpu.roll(pre[PAD : 2 * PAD], to_front, 0) + bias_i)
        all_cumulative = jnp.dot(
            jnp.concatenate(forget_rows, axis=0),
            upper,
            precision=lax.Precision.HIGHEST,
            preferred_element_type=F32,
        )
        all_in = jnp.concatenate(in_rows, axis=0)
        all_total = jnp.broadcast_to(all_cumulative[:, BLOCK - 1 : BLOCK], all_in.shape)
        exponent = all_total - all_cumulative + all_in
        all_peak = jnp.broadcast_to(jnp.max(exponent, axis=1, keepdims=True), all_in.shape)
        key_weight = jnp.exp(exponent - all_peak) * key_factor
        filler = jnp.zeros((BLOCK - 2 * PAD, BLOCK), F32)
        for j in range(n_half):
            b = index * n_half + j
            span = slice(j * PAD, (j + 1) * PAD)
            row_log[b, 0:PAD] = all_cumulative[span]
            row_log[b, PAD : 2 * PAD] = all_in[span]
            block_sum[b] = all_total[span]
            block_peak[b] = all_peak[span]
            col_log[b] = jnp.transpose(
                jnp.concatenate([all_cumulative[span], key_weight[span], filler], axis=0)
            )

    def half_state(index):
        log = jnp.full((PAD, BLOCK), LOWEST_LOG, F32)
        total = jnp.zeros((PAD, BLOCK), F32)
        filler = jnp.zeros((BLOCK - 2 * PAD, BLOCK), F32)
        keeps, adds = [], []
        for j in range(n_half):
            b = index * n_half + j
            prefix_cols[b] = jnp.transpose(jnp.concatenate([log, total, filler], axis=0))
            now, peak = block_sum[b], block_peak[b]
            merged = jnp.maximum(now + log, peak)
            keeps.append(jnp.exp(now + log - merged))
            adds.append(jnp.exp(peak - merged))
            log = merged
            total = total + now
        half_log[index] = log
        half_total[index] = total
        for h in range(heads):
            state = jnp.zeros((dh, dh), F32)
            for j in range(n_half):
                b = index * n_half + j
                rows = rows_of(b, BLOCK)
                prefix[b, h] = state.astype(BF16)
                k = k_rows[rows, head_cols(h)].astype(F32)
                wk = (col_log[b, :, PAD + h : PAD + h + 1] * k).astype(BF16)
                term = lax.dot_general(
                    wk,
                    v_rows[rows, head_cols(h)],
                    (((0,), (0,)), ((), ())),
                    preferred_element_type=F32,
                )
                state = keeps[j][h : h + 1] * state + adds[j][h : h + 1] * term
            half_sum[index, h] = state

    own_rows = rows_of(me, half)
    gate_pre[own_rows, :] = dot(normed[own_rows, :], gate_w[...])
    pl.semaphore_wait(barrier, jnp.where(place + 1 < n_sp, 2, 1))
    for c in range(n_half):
        norm_copy(c).start()

    @pl.loop(0, 2)
    def _(step):
        index = lax.rem(me + step, 2)
        rows = rows_of(index, half)

        @pl.when(step == 0)
        def _():
            w_copies[KEY].wait()

        @pl.when(step == 1)
        def _():
            for c in range(n_half):
                norm_copy(c).wait_recv()
            gate_pre[rows, :] = dot(normed[rows, :], gate_w[...])

        project(k_rows, KEY, rows)

        @pl.when(step == 0)
        def _():
            w_copies[VALUE].wait()
            for c in out_copies:
                c.start()
            for c in outw_copies:
                c.start()

        project(v_rows, VALUE, rows)
        gate_math(index)

        @pl.when(step == 0)
        def _():
            w_copies[QUERY].wait()

        project(q_rows, QUERY, rows)
        half_state(index)

    for c in w_copies[GATE_IN:]:
        c.wait()

    def state_copies(k):
        span = pl.ds(k * group, group)
        pairs = [(send_memory.at[span], carry.at[0, span], k)]
        if k == 0:
            pairs.append((send_log, carry_log.at[0], BATCHES))
        return [
            pltpu.make_async_remote_copy(
                src_ref=src,
                dst_ref=dst,
                send_sem=state_send.at[s],
                recv_sem=state_recv.at[s],
                device_id={"sp": lax.rem(place + 1, n_sp)},
                device_id_type=MESH,
            )
            for src, dst, s in pairs
        ]

    def relay(k):
        @pl.when(place > 0)
        def _():
            for c in state_copies(k):
                c.wait_recv()

        if k == 0:
            log = carry_log[0]
            for i in range(2):
                now, peak = half_total[i], half_log[i]
                merged = jnp.maximum(now + log, peak)
                relay_rows[2 * i] = jnp.exp(now + log - merged)
                relay_rows[2 * i + 1] = jnp.exp(peak - merged)
                filler = jnp.zeros((BLOCK - PAD, BLOCK), F32)
                carry_cols[i] = jnp.transpose(jnp.concatenate([log, filler], axis=0))
                log = merged
            send_log[...] = log
        for h in range(k * group, (k + 1) * group):
            state = carry[0, h].astype(F32)
            for i in range(2):
                keep = relay_rows[2 * i, h : h + 1]
                add = relay_rows[2 * i + 1, h : h + 1]
                state = keep * state + add * half_sum[i, h]
                if i == 0:
                    carry[1, h] = state.astype(BF16)
            send_memory[h] = state.astype(BF16)

        @pl.when(place + 1 < n_sp)
        def _():
            for c in state_copies(k):
                c.start()

    n_main = 2 * n_half

    def relays(g):
        for k in range(BATCHES):
            due = jnp.where(place == 0, 0, jnp.minimum(2 * place + k, n_main))

            @pl.when(due == g)
            def _(k=k):
                relay(k)

    def read_block(b):
        rows = rows_of(b, BLOCK)
        columns = col_log[b]
        carried_all = columns + prefix_cols[b]
        tops = jnp.zeros((BLOCK, BLOCK), F32)
        for h in range(heads):
            q = q_rows[rows, head_cols(h)]
            k = k_rows[rows, head_cols(h)]
            scores = lax.dot_general(
                q, k, (((1,), (1,)), ((), ())), preferred_element_type=F32
            )
            carried = dot(q, prefix[b, h])
            pair = (columns[:, h : h + 1] - row_log[b, h : h + 1]) + row_log[
                b, PAD + h : PAD + h + 1
            ]
            pair = jnp.where(causal, pair, -jnp.inf)
            carried_log = carried_all[:, h : h + 1]
            top = jnp.maximum(carried_log, jnp.max(pair, axis=1, keepdims=True))
            weighted = (jnp.exp(pair - top) * (scores * key_factor)).astype(BF16)
            local_out[rows, head_cols(h)] = jnp.exp(carried_log - top) * carried + dot(
                weighted, v_rows[rows, head_cols(h)]
            )
            tops = jnp.where(col_i == h, top, tops)
        local_top[b] = tops

    taps_cols = pl.ds(pl.multiple_of(me * width, width), width)
    taps = conv_taps[:, taps_cols].astype(F32)
    tap_count = conv_taps.shape[0]

    def product(rows):
        return (conv_pair[0, rows, :].astype(F32) * conv_pair[1, rows, :].astype(F32)).astype(BF16)

    split = n_main // 2

    @pl.loop(0, split)
    def _(g):
        relays(g)
        slot = lax.div(g, n_half // 2)
        project(conv_pair.at[slot], GATE_IN + slot, rows_of(lax.rem(g, 2), half))
        read_block(g)

    rim_out[...] = product(pl.ds(total_rows - RIM, RIM))
    rim_copy = pltpu.make_async_remote_copy(
        src_ref=rim_out,
        dst_ref=rim,
        send_sem=rim_sem.at[0],
        recv_sem=rim_sem.at[1],
        device_id={"sp": lax.rem(place + 1, n_sp)},
        device_id_type=MESH,
    )

    @pl.when(place + 1 < n_sp)
    def _():
        rim_copy.start()

    @pl.loop(split, split + 2)
    def _(g):
        relays(g)
        index = g - split
        for j in range(n_half):
            b = index * n_half + j
            target = pl.ds(pl.multiple_of(RIM + b * BLOCK, RIM), BLOCK)
            conv_rows[target, :] = product(rows_of(b, BLOCK))
        project(go_rows, GATE_OUT, rows_of(index, half))
        read_block(g)

    @pl.when(place > 0)
    def _():
        rim_copy.wait_recv()
        conv_rows[0:RIM, :] = rim[...]

    @pl.when(place == 0)
    def _():
        conv_rows[0:RIM, :] = jnp.zeros((RIM, width), BF16)

    conv_copy = partner_copy(
        mix_conv.at[1, :, pl.ds(0, width)],
        mix_conv.at[0, :, pl.ds(width, width)],
        conv_sem.at[0],
        conv_sem.at[1],
    )

    @pl.loop(split + 2, n_main)
    def _(g):
        relays(g)
        turn = g - (split + 2)
        side = jnp.where(turn == 0, other, me)
        for j in range(n_half):
            b = side * n_half + j
            x = conv_rows[pl.ds(pl.multiple_of(b * BLOCK, RIM), BLOCK + RIM), :].astype(F32)
            mixed = None
            for t in range(tap_count):
                back = tap_count - 1 - t
                y = x if back == 0 else pltpu.roll(x, back, 0)
                y = y[RIM:] * taps[t : t + 1]
                mixed = y if mixed is None else mixed + y
            mix_conv[1 - turn, pl.ds(j * BLOCK, BLOCK), pl.ds(0, width)] = (
                go_rows[rows_of(b, BLOCK), :].astype(F32) * mixed
            ).astype(BF16)
        project(og_rows, OUT_GATE, rows_of(turn, half))
        read_block(g)

        @pl.when(turn == 0)
        def _():
            conv_copy.start()

    relays(n_main)
    for c in out_copies:
        c.wait()
    for c in outw_copies:
        c.wait_recv()
    conv_copy.wait_recv()

    def finish_block(side, slot, j):
        b = side * n_half + j
        rows = rows_of(b, BLOCK)
        local = local_top[b]
        carried_all = (
            col_log[b] + pltpu.roll(prefix_cols[b], BLOCK - PAD, 1) + carry_cols[side]
        )
        top = jnp.maximum(local, carried_all)
        local_factor = jnp.exp(local - top)
        carried_factor = jnp.exp(carried_all - top)
        for h in range(heads):
            q = q_rows[rows, head_cols(h)]
            out = carried_factor[:, h : h + 1] * dot(q, carry[side, h]) + local_factor[
                :, h : h + 1
            ] * local_out[rows, head_cols(h)]
            out = out * lax.rsqrt(jnp.mean(out * out, axis=1, keepdims=True) + EPSILON)
            gate = jax.nn.sigmoid(og_rows[rows, head_cols(h)].astype(F32))
            mix_memory[slot, rows_of(j, BLOCK), head_cols(h)] = (
                out * head_rows[pl.ds(first_head + h, 1), :] * gate
            ).astype(BF16)

    def memory_copy(j):
        rows = rows_of(j, 2 * BLOCK)
        return partner_copy(
            mix_memory.at[1, rows, pl.ds(0, width)],
            mix_memory.at[0, rows, pl.ds(width, width)],
            mem_send.at[j],
            mem_recv.at[j],
        )

    early = n_out // 2

    @pl.loop(0, n_out)
    def _(j):
        slot = jnp.where(j < early, 1, 0)
        side = jnp.where(j < early, other, me)
        pair = lax.rem(j, early)
        cols = rows_of(j, out_cols)
        acc[:, cols] = dot(mix_conv[0], out_c[:, cols])
        for i in range(2):
            finish_block(side, slot, 2 * pair + i)

        @pl.when(j < early)
        def _():
            memory_copy(j).start()

    for j in range(early):
        memory_copy(j).wait_recv()

    @pl.loop(0, n_out)
    def _(j):
        cols = rows_of(j, out_cols)
        layer_out[:, cols] = (acc[:, cols] + dot(mix_memory[0], out_m[:, cols])).astype(BF16)

    for c in range(n_half):
        norm_copy(c).wait_send()
    for c in outw_copies:
        c.wait_send()
    conv_copy.wait_send()
    for j in range(early):
        memory_copy(j).wait_send()

    @pl.when(place + 1 < n_sp)
    def _():
        rim_copy.wait_send()
        for k in range(BATCHES):
            for c in state_copies(k):
                c.wait_send()


def local(
    tokens,
    norm_gain,
    w_query,
    w_key,
    w_value,
    w_outgate,
    w_gatein,
    w_gateout,
    w_convin,
    w_igate,
    w_fgate,
    input_bias,
    forget_bias,
    forget_extra,
    init_memory,
    head_gain,
    conv_taps,
    out_memory,
    out_conv,
):
    heads, dh = init_memory.shape[1], init_memory.shape[2]
    half, features = tokens.shape[1], tokens.shape[2]
    rows = forget_extra.shape[1]
    width = w_query.shape[1]
    nblocks = rows // BLOCK
    n_half = half // BLOCK
    all_heads = w_igate.shape[1]
    n_sp = lax.axis_size("sp")
    hbm = pl.BlockSpec(memory_space=pl.ANY)
    dma = pltpu.SemaphoreType.DMA
    out = pl.pallas_call(
        functools.partial(kernel, n_sp),
        name="layer",
        out_shape=pltpu.VMEM((half, features), BF16),
        in_specs=[hbm] * 19,
        out_specs=pl.BlockSpec(memory_space=pltpu.VMEM),
        scratch_shapes=[
            pltpu.VMEM((half, features), BF16),
            pltpu.VMEM((features // BLOCK, BLOCK), BF16),
            pltpu.VMEM((1, features), F32),
            pltpu.VMEM((all_heads, dh), BF16),
            pltpu.VMEM((all_heads, dh), F32),
            pltpu.VMEM((all_heads, features), BF16),
            pltpu.VMEM((all_heads, features), BF16),
            pltpu.VMEM((features, BLOCK), BF16),
            pltpu.SMEM((2, all_heads), F32),
            pltpu.VMEM((heads, rows), F32),
            pltpu.VMEM((heads, dh, dh), F32),
            pltpu.VMEM(conv_taps.shape, BF16),
            pltpu.VMEM((rows, features), BF16),
            pltpu.VMEM((7, features, width), BF16),
            pltpu.VMEM((2 * width, features), BF16),
            pltpu.VMEM((2 * width, features), BF16),
            pltpu.VMEM((rows, width), BF16),
            pltpu.VMEM((rows, width), BF16),
            pltpu.VMEM((rows, width), BF16),
            pltpu.VMEM((2, rows, width), BF16),
            pltpu.VMEM((rows, width), BF16),
            pltpu.VMEM((rows, width), BF16),
            pltpu.VMEM((rows, BLOCK), F32),
            pltpu.VMEM((nblocks, 2 * PAD, BLOCK), F32),
            pltpu.VMEM((nblocks, BLOCK, BLOCK), F32),
            pltpu.VMEM((nblocks, PAD, BLOCK), F32),
            pltpu.VMEM((nblocks, PAD, BLOCK), F32),
            pltpu.VMEM((nblocks, heads, dh, dh), BF16),
            pltpu.VMEM((nblocks, BLOCK, BLOCK), F32),
            pltpu.VMEM((2, heads, dh, dh), F32),
            pltpu.VMEM((2, PAD, BLOCK), F32),
            pltpu.VMEM((2, PAD, BLOCK), F32),
            pltpu.VMEM((4, PAD, BLOCK), F32),
            pltpu.VMEM((2, heads, dh, dh), BF16),
            pltpu.VMEM((2, PAD, BLOCK), F32),
            pltpu.VMEM((2, BLOCK, BLOCK), F32),
            pltpu.VMEM((heads, dh, dh), BF16),
            pltpu.VMEM((PAD, BLOCK), F32),
            pltpu.VMEM((rows, width), F32),
            pltpu.VMEM((nblocks, BLOCK, BLOCK), F32),
            pltpu.VMEM((RIM + rows, width), BF16),
            pltpu.VMEM((RIM, width), BF16),
            pltpu.VMEM((RIM, width), BF16),
            pltpu.VMEM((2, half, 2 * width), BF16),
            pltpu.VMEM((2, half, 2 * width), BF16),
            pltpu.VMEM((half, features), F32),
            dma((n_half,)),
            dma((9,)),
            dma((9,)),
            dma((n_half,)),
            dma((n_half,)),
            dma((2,)),
            dma((2,)),
            dma((BATCHES + 1,)),
            dma((BATCHES + 1,)),
            dma((2,)),
            dma((2,)),
            dma((n_half // 2,)),
            dma((n_half // 2,)),
        ],
        compiler_params=pltpu.CompilerParams(
            collective_id=0, has_side_effects=True, vmem_limit_bytes=60 * 1024 * 1024
        ),
    )(
        tokens[0],
        norm_gain.reshape(-1, BLOCK),
        w_key,
        w_value,
        w_query,
        w_gatein,
        w_convin,
        w_gateout,
        w_outgate,
        jnp.transpose(w_igate),
        jnp.transpose(w_fgate),
        input_bias,
        forget_bias,
        jnp.transpose(forget_extra[0]),
        init_memory[0],
        head_gain.reshape(-1, dh),
        conv_taps,
        out_memory,
        out_conv,
    )
    return out[None]


def solution(mesh):
    return jax.shard_map(
        local,
        mesh=mesh,
        in_specs=(
            P("fs", ("sp", "tp"), None),
            P(),
            P(None, "tp"),
            P(None, "tp"),
            P(None, "tp"),
            P(None, "tp"),
            P(None, "tp"),
            P(None, "tp"),
            P(None, "tp"),
            P(),
            P(),
            P(),
            P(),
            P("fs", "sp", "tp"),
            P("fs", "tp", None, None),
            P(),
            P(),
            P("tp", None),
            P("tp", None),
        ),
        out_specs=P("fs", ("sp", "tp"), None),
        check_vma=False,
    )
```

```python
import functools

import jax
import jax.numpy as jnp
from jax import lax
from jax.experimental import pallas as pl
from jax.experimental.pallas import tpu as pltpu
from jax.sharding import PartitionSpec as P

BLOCK = 128
EPSILON = 1e-06
LOWEST_LOG = -1e30
MESH = pl.DeviceIdType.MESH
F32 = jnp.float32
BF16 = jnp.bfloat16
PAD = 8
RIM = 8
NORM_ROWS = 64
BATCHES = 2
PARTS = 2

KEY, VALUE, QUERY, GATE_IN, CONV_IN, GATE_OUT, OUT_GATE = range(7)


def kernel(
    n_sp,
    tokens,
    norm_gain,
    w_key,
    w_value,
    w_query,
    w_gatein,
    w_convin,
    w_gateout,
    w_outgate,
    w_igate,
    w_fgate,
    input_bias,
    forget_bias,
    extra_in,
    init_in,
    head_gain,
    taps_in,
    out_memory,
    out_conv,
    layer_out,
    tok,
    gain_in,
    gain_row,
    head_in,
    head_rows,
    igate_in,
    fgate_in,
    gate_w,
    bias_in,
    extra,
    init_memory,
    conv_taps,
    normed,
    weights,
    out_m,
    out_c,
    k_rows,
    v_rows,
    q_rows,
    conv_pair,
    go_rows,
    og_rows,
    gate_pre,
    row_log,
    col_log,
    block_sum,
    block_peak,
    prefix,
    prefix_cols,
    half_sum,
    half_log,
    half_total,
    relay_rows,
    carry,
    carry_log,
    carry_cols,
    send_memory,
    send_log,
    local_out,
    local_top,
    conv_rows,
    rim,
    rim_out,
    mix_conv,
    mix_memory,
    acc,
    token_sem,
    small_sem,
    weight_sem,
    norm_send,
    norm_recv,
    outw_send,
    outw_recv,
    state_send,
    state_recv,
    rim_sem,
    conv_sem,
    mem_send,
    mem_recv,
):
    me = lax.axis_index("tp")
    other = 1 - me
    place = lax.axis_index("sp")
    half = tok.shape[0]
    total_rows = normed.shape[0]
    width = k_rows.shape[1]
    heads = init_memory.shape[0]
    dh = init_memory.shape[1]
    n_half = half // BLOCK
    nblocks = total_rows // BLOCK
    key_factor = dh ** (-0.5)
    out_width = layer_out.shape[1]
    group = heads // BATCHES

    barrier = pltpu.get_barrier_semaphore()
    pl.semaphore_signal(barrier, inc=1, device_id={"tp": other}, device_id_type=MESH)

    @pl.when(place > 0)
    def _():
        pl.semaphore_signal(barrier, inc=1, device_id={"sp": place - 1}, device_id_type=MESH)

    def rows_of(index, size):
        return pl.ds(pl.multiple_of(index * size, size), size)

    tok_copies = [
        pltpu.make_async_copy(
            tokens.at[pl.ds(c * BLOCK, BLOCK)], tok.at[pl.ds(c * BLOCK, BLOCK)], token_sem.at[c]
        )
        for c in range(n_half)
    ]
    smalls = [
        pltpu.make_async_copy(src, dst, small_sem.at[i])
        for i, (src, dst) in enumerate(
            (
                (norm_gain, gain_in),
                (w_igate, igate_in),
                (w_fgate, fgate_in),
                (input_bias, bias_in.at[0]),
                (forget_bias, bias_in.at[1]),
                (extra_in, extra),
                (init_in, init_memory),
                (head_gain, head_in),
                (taps_in, conv_taps),
            )
        )
    ]
    w_in = (w_key, w_value, w_query, w_gatein, w_convin, w_gateout, w_outgate)
    w_copies = [
        pltpu.make_async_copy(w, weights.at[s], weight_sem.at[s]) for s, w in enumerate(w_in)
    ]
    out_copies = [
        pltpu.make_async_copy(out_memory, out_m.at[pl.ds(0, width)], weight_sem.at[7]),
        pltpu.make_async_copy(out_conv, out_c.at[pl.ds(0, width)], weight_sem.at[8]),
    ]

    def partner_copy(src, dst, send_sem, recv_sem):
        return pltpu.make_async_remote_copy(
            src_ref=src,
            dst_ref=dst,
            send_sem=send_sem,
            recv_sem=recv_sem,
            device_id={"tp": other},
            device_id_type=MESH,
        )

    def norm_copy(c):
        rows = pl.ds(pl.multiple_of(me * half + c * BLOCK, BLOCK), BLOCK)
        return partner_copy(normed.at[rows], normed.at[rows], norm_send.at[c], norm_recv.at[c])

    outw_copies = [
        partner_copy(src, dst.at[pl.ds(width, width)], outw_send.at[i], outw_recv.at[i])
        for i, (src, dst) in enumerate(((out_conv, out_c), (out_memory, out_m)))
    ]

    smalls[0].start()
    for c in tok_copies:
        c.start()
    for c in smalls[1:]:
        c.start()

    smalls[0].wait()
    for j in range(norm_gain.shape[0]):
        gain_row[:, j * BLOCK : (j + 1) * BLOCK] = gain_in[j : j + 1].astype(F32)

    def normalize(c):
        for part in range(BLOCK // NORM_ROWS):
            start = c * BLOCK + part * NORM_ROWS
            x = tok[pl.ds(start, NORM_ROWS), :].astype(F32)
            scale = lax.rsqrt(jnp.mean(x * x, axis=-1, keepdims=True) + EPSILON)
            y = (x * scale) * gain_row[...]
            normed[pl.ds(pl.multiple_of(me * half + start, NORM_ROWS), NORM_ROWS), :] = y.astype(
                BF16
            )

    def gate_dot(c):
        rows = pl.ds(pl.multiple_of(me * half + c * BLOCK, BLOCK), BLOCK)
        gate_pre[rows, :] = jnp.dot(
            normed[rows, :], gate_w[...], preferred_element_type=F32
        )

    first_weights = 3
    smalls[1].wait()
    smalls[2].wait()
    gates = jnp.concatenate(
        [
            fgate_in[...],
            igate_in[...],
            jnp.zeros((BLOCK - 2 * PAD, igate_in.shape[1]), BF16),
        ],
        axis=0,
    )
    gate_w[...] = jnp.transpose(gates)
    for c in range(n_half):
        tok_copies[c].wait()
        if c < first_weights:
            w_copies[c].start()
        if c > 0:
            gate_dot(c - 1)
        normalize(c)
    for c in w_copies[min(first_weights, n_half) :]:
        c.start()

    for c in smalls[3:]:
        c.wait()
    head_rows[...] = head_in[...].astype(F32)

    @pl.when(place == 0)
    def _():
        for h in range(heads):
            carry[0, h] = init_memory[h].astype(BF16)
        carry_log[0] = jnp.zeros((PAD, BLOCK), F32)

    row_i = lax.broadcasted_iota(jnp.int32, (BLOCK, BLOCK), 0)
    col_i = lax.broadcasted_iota(jnp.int32, (BLOCK, BLOCK), 1)
    upper = jnp.where(row_i <= col_i, 1.0, 0.0).astype(F32)
    causal = col_i <= row_i

    def head_cols(h):
        return slice(h * dh, (h + 1) * dh)

    first_head = me * heads
    to_front = lax.rem(PAD - first_head, PAD)
    lane_head = lax.broadcasted_iota(jnp.int32, (PAD, BLOCK), 0)
    bias_f = jnp.zeros((PAD, BLOCK), F32)
    bias_i = jnp.zeros((PAD, BLOCK), F32)
    for h in range(heads):
        bias_i = jnp.where(lane_head == h, bias_in[0, first_head + h], bias_i)
        bias_f = jnp.where(lane_head == h, bias_in[1, first_head + h], bias_f)
    no_head = jnp.zeros((PAD - heads, BLOCK), F32)

    def dot(a, b):
        return jnp.dot(a, b, preferred_element_type=F32)

    def project(target, slot, index, part):
        size = half // PARTS
        rows = rows_of(index * PARTS + part, size)
        target[rows, :] = dot(normed[rows, :], weights[slot]).astype(BF16)

    def gate_sums(index):
        forget_rows, in_rows = [], []
        for j in range(n_half):
            span = rows_of(index * n_half + j, BLOCK)
            pre = jnp.transpose(gate_pre[span, :])
            v = pltpu.roll(pre[0:PAD], to_front, 0) + bias_f
            log_forget = jnp.minimum(v, 0.0) - jnp.log1p(jnp.exp(-jnp.abs(v)))
            forget_rows.append(log_forget + jnp.concatenate([extra[:, span], no_head], axis=0))
            in_rows.append(pltpu.roll(pre[PAD : 2 * PAD], to_front, 0) + bias_i)
        all_cumulative = jnp.dot(
            jnp.concatenate(forget_rows, axis=0),
            upper,
            precision=lax.Precision.HIGHEST,
            preferred_element_type=F32,
        )
        return all_cumulative, jnp.concatenate(in_rows, axis=0)

    def gate_logs(index, all_cumulative, all_in):
        all_total = jnp.broadcast_to(all_cumulative[:, BLOCK - 1 : BLOCK], all_in.shape)
        exponent = all_total - all_cumulative + all_in
        all_peak = jnp.broadcast_to(jnp.max(exponent, axis=1, keepdims=True), all_in.shape)
        key_weight = jnp.exp(exponent - all_peak) * key_factor
        filler = jnp.zeros((BLOCK - 2 * PAD, BLOCK), F32)
        for j in range(n_half):
            b = index * n_half + j
            span = slice(j * PAD, (j + 1) * PAD)
            row_log[b, 0:PAD] = all_cumulative[span]
            row_log[b, PAD : 2 * PAD] = all_in[span]
            block_sum[b] = all_total[span]
            block_peak[b] = all_peak[span]
            col_log[b] = jnp.transpose(
                jnp.concatenate([all_cumulative[span], key_weight[span], filler], axis=0)
            )

    def block_terms(index):
        terms = []
        for h in range(heads):
            for j in range(n_half):
                b = index * n_half + j
                rows = rows_of(b, BLOCK)
                k = k_rows[rows, head_cols(h)].astype(F32)
                wk = (col_log[b, :, PAD + h : PAD + h + 1] * k).astype(BF16)
                terms.append(
                    lax.dot_general(
                        wk,
                        v_rows[rows, head_cols(h)],
                        (((0,), (0,)), ((), ())),
                        preferred_element_type=F32,
                    )
                )
        return terms

    def half_state(index, terms):
        log = jnp.full((PAD, BLOCK), LOWEST_LOG, F32)
        total = jnp.zeros((PAD, BLOCK), F32)
        filler = jnp.zeros((BLOCK - 2 * PAD, BLOCK), F32)
        keeps, adds = [], []
        for j in range(n_half):
            b = index * n_half + j
            prefix_cols[b] = jnp.transpose(jnp.concatenate([log, total, filler], axis=0))
            now, peak = block_sum[b], block_peak[b]
            merged = jnp.maximum(now + log, peak)
            keeps.append(jnp.exp(now + log - merged))
            adds.append(jnp.exp(peak - merged))
            log = merged
            total = total + now
        half_log[index] = log
        half_total[index] = total
        for h in range(heads):
            state = jnp.zeros((dh, dh), F32)
            for j in range(n_half):
                prefix[index * n_half + j, h] = state.astype(BF16)
                state = (
                    keeps[j][h : h + 1] * state + adds[j][h : h + 1] * terms[h * n_half + j]
                )
            half_sum[index, h] = state

    def keys(index):
        for p in range(PARTS):
            project(k_rows, KEY, index, p)

    def values_queries(index):
        project(v_rows, VALUE, index, 0)
        sums = gate_sums(index)
        project(v_rows, VALUE, index, 1)
        gate_logs(index, *sums)
        project(q_rows, QUERY, index, 0)
        terms = block_terms(index)
        project(q_rows, QUERY, index, 1)
        half_state(index, terms)

    once = jnp.minimum(place + 1, 1)

    def region(body):
        pl.loop(0, once)(lambda _: body())

    pl.semaphore_wait(barrier, jnp.where(place + 1 < n_sp, 2, 1))
    for c in range(n_half):
        norm_copy(c).start()
    w_copies[KEY].wait()
    @region
    def _():
        gate_dot(n_half - 1)
        keys(me)

    w_copies[VALUE].wait()
    w_copies[QUERY].wait()
    for c in out_copies:
        c.start()
    for c in outw_copies:
        c.start()
    @region
    def _():
        values_queries(me)

    for c in range(n_half):
        norm_copy(c).wait_recv()
    @region
    def _():
        other_rows = rows_of(other, half)
        gate_pre[other_rows, :] = dot(normed[other_rows, :], gate_w[...])
        keys(other)
        values_queries(other)

    for c in w_copies[GATE_IN:]:
        c.wait()

    def state_copies(k):
        span = pl.ds(k * group, group)
        pairs = [(send_memory.at[span], carry.at[0, span], k)]
        if k == 0:
            pairs.append((send_log, carry_log.at[0], BATCHES))
        return [
            pltpu.make_async_remote_copy(
                src_ref=src,
                dst_ref=dst,
                send_sem=state_send.at[s],
                recv_sem=state_recv.at[s],
                device_id={"sp": lax.rem(place + 1, n_sp)},
                device_id_type=MESH,
            )
            for src, dst, s in pairs
        ]

    def relay(k):
        @pl.when(place > 0)
        def _():
            for c in state_copies(k):
                c.wait_recv()

        if k == 0:
            log = carry_log[0]
            for i in range(2):
                now, peak = half_total[i], half_log[i]
                merged = jnp.maximum(now + log, peak)
                relay_rows[2 * i] = jnp.exp(now + log - merged)
                relay_rows[2 * i + 1] = jnp.exp(peak - merged)
                filler = jnp.zeros((BLOCK - PAD, BLOCK), F32)
                carry_cols[i] = jnp.transpose(jnp.concatenate([log, filler], axis=0))
                log = merged
            send_log[...] = log
        for h in range(k * group, (k + 1) * group):
            state = carry[0, h].astype(F32)
            for i in range(2):
                keep = relay_rows[2 * i, h : h + 1]
                add = relay_rows[2 * i + 1, h : h + 1]
                state = keep * state + add * half_sum[i, h]
                if i == 0:
                    carry[1, h] = state.astype(BF16)
            send_memory[h] = state.astype(BF16)

        @pl.when(place + 1 < n_sp)
        def _():
            for c in state_copies(k):
                c.start()

    n_main = 2 * n_half

    def relays(g):
        for k in range(BATCHES):
            due = jnp.where(place == 0, 0, jnp.minimum(2 * place + 1 + k, n_main))

            @pl.when(due == g)
            def _(k=k):
                relay(k)

    def read_scores(b):
        rows = rows_of(b, BLOCK)
        return [
            lax.dot_general(
                q_rows[rows, head_cols(h)],
                k_rows[rows, head_cols(h)],
                (((1,), (1,)), ((), ())),
                preferred_element_type=F32,
            )
            for h in range(heads)
        ]

    def read_values(b, scores):
        rows = rows_of(b, BLOCK)
        columns = col_log[b]
        carried_all = columns + prefix_cols[b]
        tops = jnp.zeros((BLOCK, BLOCK), F32)
        for h in range(heads):
            pair = (columns[:, h : h + 1] - row_log[b, h : h + 1]) + row_log[
                b, PAD + h : PAD + h + 1
            ]
            pair = jnp.where(causal, pair, -jnp.inf)
            carried_log = carried_all[:, h : h + 1]
            top = jnp.maximum(carried_log, jnp.max(pair, axis=1, keepdims=True))
            weighted = (jnp.exp(pair - top) * (scores[h] * key_factor)).astype(BF16)
            q = q_rows[rows, head_cols(h)].astype(F32)
            carried = (jnp.exp(carried_log - top) * q).astype(BF16)
            local_out[rows, head_cols(h)] = dot(
                jnp.concatenate([weighted, carried], axis=1),
                jnp.concatenate([v_rows[rows, head_cols(h)], prefix[b, h]], axis=0),
            )
            tops = jnp.where(col_i == h, top, tops)
        local_top[b] = tops

    taps_cols = pl.ds(pl.multiple_of(me * width, width), width)
    taps = conv_taps[:, taps_cols].astype(F32)
    tap_count = conv_taps.shape[0]

    def product(rows, cols):
        return conv_pair[0, rows, cols].astype(F32) * conv_pair[1, rows, cols].astype(F32)

    def products(b):
        target = pl.ds(pl.multiple_of(RIM + b * BLOCK, RIM), BLOCK)
        for h in range(heads):
            conv_rows[h, target, :] = product(rows_of(b, BLOCK), head_cols(h))

    def convolve(b, slot, j):
        for h in range(heads):
            cols = head_cols(h)
            mixed = None
            for t in range(tap_count):
                x = conv_rows[h, pl.ds(b * BLOCK + (RIM - tap_count + 1 + t), BLOCK), :]
                y = x * taps[t : t + 1, cols]
                mixed = y if mixed is None else mixed + y
            mix_conv[slot, pl.ds(j * BLOCK, BLOCK), cols] = (
                go_rows[rows_of(b, BLOCK), cols].astype(F32) * mixed
            ).astype(BF16)

    split = n_main // 2

    @pl.loop(0, split)
    def _(g):
        relays(g)
        slot = lax.div(g, n_half // 2)
        index = lax.rem(g, 2)
        scores = read_scores(g)
        project(conv_pair.at[slot], GATE_IN + slot, index, 0)
        read_values(g, scores)
        project(conv_pair.at[slot], GATE_IN + slot, index, 1)

    for h in range(heads):
        rim_out[h] = product(pl.ds(total_rows - 2 * RIM, 2 * RIM), head_cols(h))[RIM:]
    rim_copy = pltpu.make_async_remote_copy(
        src_ref=rim_out,
        dst_ref=rim,
        send_sem=rim_sem.at[0],
        recv_sem=rim_sem.at[1],
        device_id={"sp": lax.rem(place + 1, n_sp)},
        device_id_type=MESH,
    )

    @pl.when(place + 1 < n_sp)
    def _():
        rim_copy.start()

    @pl.loop(split, split + 2)
    def _(g):
        relays(g)
        index = g - split
        scores = read_scores(g)
        project(go_rows, GATE_OUT, index, 0)
        read_values(g, scores)
        for j in range(n_half):
            products(index * n_half + j)
        project(go_rows, GATE_OUT, index, 1)

    @pl.when(place > 0)
    def _():
        rim_copy.wait_recv()
        conv_rows[:, 0:RIM, :] = rim[...]

    @pl.when(place == 0)
    def _():
        conv_rows[:, 0:RIM, :] = jnp.zeros((heads, RIM, dh), F32)

    conv_copy = partner_copy(
        mix_conv.at[1, :, pl.ds(0, width)],
        mix_conv.at[0, :, pl.ds(width, width)],
        conv_sem.at[0],
        conv_sem.at[1],
    )

    @pl.loop(split + 2, n_main)
    def _(g):
        relays(g)
        turn = g - (split + 2)
        side = jnp.where(turn == 0, other, me)
        scores = read_scores(g)
        project(og_rows, OUT_GATE, turn, 0)
        read_values(g, scores)
        for j in range(n_half):
            convolve(side * n_half + j, 1 - turn, j)
        project(og_rows, OUT_GATE, turn, 1)

        @pl.when(turn == 0)
        def _():
            conv_copy.start()

    relays(n_main)
    for c in out_copies:
        c.wait()
    for c in outw_copies:
        c.wait_recv()
    conv_copy.wait_recv()

    def finish_dots(side, j):
        rows = rows_of(side * n_half + j, BLOCK)
        return [dot(q_rows[rows, head_cols(h)], carry[side, h]) for h in range(heads)]

    def finish_block(side, slot, j, carried):
        b = side * n_half + j
        rows = rows_of(b, BLOCK)
        local = local_top[b]
        carried_all = (
            col_log[b] + pltpu.roll(prefix_cols[b], BLOCK - PAD, 1) + carry_cols[side]
        )
        top = jnp.maximum(local, carried_all)
        local_factor = jnp.exp(local - top)
        carried_factor = jnp.exp(carried_all - top)
        for h in range(heads):
            out = carried_factor[:, h : h + 1] * carried[h] + local_factor[
                :, h : h + 1
            ] * local_out[rows, head_cols(h)]
            out = out * lax.rsqrt(jnp.mean(out * out, axis=1, keepdims=True) + EPSILON)
            gate = jax.nn.sigmoid(og_rows[rows, head_cols(h)].astype(F32))
            mix_memory[slot, rows_of(j, BLOCK), head_cols(h)] = (
                out * head_rows[pl.ds(first_head + h, 1), :] * gate
            ).astype(BF16)

    def memory_copy(j):
        rows = rows_of(j, BLOCK)
        return partner_copy(
            mix_memory.at[1, rows, pl.ds(0, width)],
            mix_memory.at[0, rows, pl.ds(width, width)],
            mem_send.at[j],
            mem_recv.at[j],
        )

    wide = out_width // 2

    @pl.loop(0, 2)
    def _(turn):
        side = jnp.where(turn == 0, other, me)
        cols = rows_of(turn, wide)
        size = half // PARTS
        carried = [finish_dots(side, j) for j in range(n_half)]
        for p in range(PARTS):
            rows = slice(p * size, (p + 1) * size)
            acc[rows, cols] = dot(mix_conv[0, rows, :], out_c[:, cols])
            for j in range(p * n_half // PARTS, (p + 1) * n_half // PARTS):
                finish_block(side, 1 - turn, j, carried[j])

        @pl.when(turn == 0)
        def _():
            for j in range(n_half):
                memory_copy(j).start()

    @region
    def _():
        acc[...] += dot(mix_memory[0, :, 0:width], out_m[0:width, :])

    for j in range(n_half):
        memory_copy(j).wait_recv()

    @region
    def _():
        layer_out[...] = (
            acc[...] + dot(mix_memory[0, :, width:], out_m[pl.ds(width, width), :])
        ).astype(BF16)

    for c in range(n_half):
        norm_copy(c).wait_send()
    for c in outw_copies:
        c.wait_send()
    conv_copy.wait_send()
    for j in range(n_half):
        memory_copy(j).wait_send()

    @pl.when(place + 1 < n_sp)
    def _():
        rim_copy.wait_send()
        for k in range(BATCHES):
            for c in state_copies(k):
                c.wait_send()


def local(
    tokens,
    norm_gain,
    w_query,
    w_key,
    w_value,
    w_outgate,
    w_gatein,
    w_gateout,
    w_convin,
    w_igate,
    w_fgate,
    input_bias,
    forget_bias,
    forget_extra,
    init_memory,
    head_gain,
    conv_taps,
    out_memory,
    out_conv,
):
    heads, dh = init_memory.shape[1], init_memory.shape[2]
    half, features = tokens.shape[1], tokens.shape[2]
    rows = forget_extra.shape[1]
    width = w_query.shape[1]
    nblocks = rows // BLOCK
    n_half = half // BLOCK
    all_heads = w_igate.shape[1]
    n_sp = lax.axis_size("sp")
    hbm = pl.BlockSpec(memory_space=pl.ANY)
    dma = pltpu.SemaphoreType.DMA
    out = pl.pallas_call(
        functools.partial(kernel, n_sp),
        name="layer",
        out_shape=pltpu.VMEM((half, features), BF16),
        in_specs=[hbm] * 19,
        out_specs=pl.BlockSpec(memory_space=pltpu.VMEM),
        scratch_shapes=[
            pltpu.VMEM((half, features), BF16),
            pltpu.VMEM((features // BLOCK, BLOCK), BF16),
            pltpu.VMEM((1, features), F32),
            pltpu.VMEM((all_heads, dh), BF16),
            pltpu.VMEM((all_heads, dh), F32),
            pltpu.VMEM((all_heads, features), BF16),
            pltpu.VMEM((all_heads, features), BF16),
            pltpu.VMEM((features, BLOCK), BF16),
            pltpu.SMEM((2, all_heads), F32),
            pltpu.VMEM((heads, rows), F32),
            pltpu.VMEM((heads, dh, dh), F32),
            pltpu.VMEM(conv_taps.shape, BF16),
            pltpu.VMEM((rows, features), BF16),
            pltpu.VMEM((7, features, width), BF16),
            pltpu.VMEM((2 * width, features), BF16),
            pltpu.VMEM((2 * width, features), BF16),
            pltpu.VMEM((rows, width), BF16),
            pltpu.VMEM((rows, width), BF16),
            pltpu.VMEM((rows, width), BF16),
            pltpu.VMEM((2, rows, width), BF16),
            pltpu.VMEM((rows, width), BF16),
            pltpu.VMEM((rows, width), BF16),
            pltpu.VMEM((rows, BLOCK), F32),
            pltpu.VMEM((nblocks, 2 * PAD, BLOCK), F32),
            pltpu.VMEM((nblocks, BLOCK, BLOCK), F32),
            pltpu.VMEM((nblocks, PAD, BLOCK), F32),
            pltpu.VMEM((nblocks, PAD, BLOCK), F32),
            pltpu.VMEM((nblocks, heads, dh, dh), BF16),
            pltpu.VMEM((nblocks, BLOCK, BLOCK), F32),
            pltpu.VMEM((2, heads, dh, dh), F32),
            pltpu.VMEM((2, PAD, BLOCK), F32),
            pltpu.VMEM((2, PAD, BLOCK), F32),
            pltpu.VMEM((4, PAD, BLOCK), F32),
            pltpu.VMEM((2, heads, dh, dh), BF16),
            pltpu.VMEM((2, PAD, BLOCK), F32),
            pltpu.VMEM((2, BLOCK, BLOCK), F32),
            pltpu.VMEM((heads, dh, dh), BF16),
            pltpu.VMEM((PAD, BLOCK), F32),
            pltpu.VMEM((rows, width), F32),
            pltpu.VMEM((nblocks, BLOCK, BLOCK), F32),
            pltpu.VMEM((heads, RIM + rows, dh), F32),
            pltpu.VMEM((heads, RIM, dh), F32),
            pltpu.VMEM((heads, RIM, dh), F32),
            pltpu.VMEM((2, half, 2 * width), BF16),
            pltpu.VMEM((2, half, 2 * width), BF16),
            pltpu.VMEM((half, features), F32),
            dma((n_half,)),
            dma((9,)),
            dma((9,)),
            dma((n_half,)),
            dma((n_half,)),
            dma((2,)),
            dma((2,)),
            dma((BATCHES + 1,)),
            dma((BATCHES + 1,)),
            dma((2,)),
            dma((2,)),
            dma((n_half,)),
            dma((n_half,)),
        ],
        compiler_params=pltpu.CompilerParams(
            collective_id=0, has_side_effects=True, vmem_limit_bytes=60 * 1024 * 1024
        ),
    )(
        tokens[0],
        norm_gain.reshape(-1, BLOCK),
        w_key,
        w_value,
        w_query,
        w_gatein,
        w_convin,
        w_gateout,
        w_outgate,
        jnp.transpose(w_igate),
        jnp.transpose(w_fgate),
        input_bias,
        forget_bias,
        jnp.transpose(forget_extra[0]),
        init_memory[0],
        head_gain.reshape(-1, dh),
        conv_taps,
        out_memory,
        out_conv,
    )
    return out[None]


def solution(mesh):
    return jax.shard_map(
        local,
        mesh=mesh,
        in_specs=(
            P("fs", ("sp", "tp"), None),
            P(),
            P(None, "tp"),
            P(None, "tp"),
            P(None, "tp"),
            P(None, "tp"),
            P(None, "tp"),
            P(None, "tp"),
            P(None, "tp"),
            P(),
            P(),
            P(),
            P(),
            P("fs", "sp", "tp"),
            P("fs", "tp", None, None),
            P(),
            P(),
            P("tp", None),
            P("tp", None),
        ),
        out_specs=P("fs", ("sp", "tp"), None),
        check_vma=False,
    )
```

```python
import functools

import jax
import jax.numpy as jnp
from jax import lax
from jax.experimental import pallas as pl
from jax.experimental.pallas import tpu as pltpu
from jax.sharding import PartitionSpec as P

BLOCK = 128
EPSILON = 1e-06
LOWEST_LOG = -1e30
MESH = pl.DeviceIdType.MESH
F32 = jnp.float32
BF16 = jnp.bfloat16
PAD = 8
RIM = 8
NORM_ROWS = 64
BATCHES = 2
PARTS = 2

KEY, VALUE, QUERY, GATE_IN, CONV_IN, GATE_OUT, OUT_GATE = range(7)


def kernel(
    n_sp,
    tokens,
    norm_gain,
    w_key,
    w_value,
    w_query,
    w_gatein,
    w_convin,
    w_gateout,
    w_outgate,
    w_igate,
    w_fgate,
    input_bias,
    forget_bias,
    extra_in,
    init_in,
    head_gain,
    taps_in,
    out_memory,
    out_conv,
    layer_out,
    tok,
    gain_in,
    gain_row,
    head_in,
    head_rows,
    igate_in,
    fgate_in,
    gate_w,
    bias_in,
    extra,
    init_memory,
    conv_taps,
    normed,
    weights,
    out_m,
    out_c,
    k_rows,
    v_rows,
    q_rows,
    conv_pair,
    go_rows,
    og_rows,
    gate_pre,
    row_log,
    col_log,
    block_sum,
    block_peak,
    prefix,
    prefix_cols,
    total_cols,
    half_sum,
    half_log,
    half_total,
    relay_rows,
    carry,
    carry_log,
    carry_cols,
    send_memory,
    send_log,
    local_out,
    local_top,
    conv_rows,
    rim,
    rim_out,
    mix_conv,
    mix_memory,
    acc,
    token_sem,
    small_sem,
    weight_sem,
    norm_send,
    norm_recv,
    outw_send,
    outw_recv,
    state_send,
    state_recv,
    ready,
    rim_sem,
    conv_sem,
    mem_send,
    mem_recv,
):
    me = lax.axis_index("tp")
    other = 1 - me
    place = lax.axis_index("sp")
    half = tok.shape[0]
    total_rows = normed.shape[0]
    width = k_rows.shape[1]
    heads = init_memory.shape[0]
    dh = init_memory.shape[1]
    n_half = half // BLOCK
    nblocks = total_rows // BLOCK
    key_factor = dh ** (-0.5)
    out_width = layer_out.shape[1]
    group = heads // BATCHES
    chunks, piece = out_c.shape[0], out_c.shape[2]

    barrier = pltpu.get_barrier_semaphore()
    pl.semaphore_signal(barrier, inc=1, device_id={"tp": other}, device_id_type=MESH)

    @pl.when(place + 1 < n_sp)
    def _():
        pl.semaphore_signal(barrier, inc=1, device_id={"sp": place + 1}, device_id_type=MESH)

    def head_cols(h):
        return slice(h * dh, (h + 1) * dh)

    def rows_of(index, size):
        return pl.ds(pl.multiple_of(index * size, size), size)

    tok_copies = [
        pltpu.make_async_copy(
            tokens.at[pl.ds(c * BLOCK, BLOCK)], tok.at[pl.ds(c * BLOCK, BLOCK)], token_sem.at[c]
        )
        for c in range(n_half)
    ]
    smalls = [
        pltpu.make_async_copy(src, dst, small_sem.at[i])
        for i, (src, dst) in enumerate(
            (
                (norm_gain, gain_in),
                (w_igate, igate_in),
                (w_fgate, fgate_in),
                (input_bias, bias_in.at[0]),
                (forget_bias, bias_in.at[1]),
                (extra_in, extra),
                (init_in, init_memory),
                (head_gain, head_in),
                (taps_in, conv_taps),
            )
        )
    ]
    w_in = (w_key, w_value, w_query, w_gatein, w_convin, w_gateout, w_outgate)
    w_copies = [
        pltpu.make_async_copy(w, weights.at[s], weight_sem.at[s]) for s, w in enumerate(w_in)
    ]
    out_copies = [
        pltpu.make_async_copy(out_memory, out_m.at[pl.ds(0, width)], weight_sem.at[7]),
    ] + [
        pltpu.make_async_copy(
            out_conv.at[:, pl.ds(c * piece, piece)], out_c.at[c, pl.ds(0, width)], weight_sem.at[8 + c]
        )
        for c in range(chunks)
    ]

    def partner_copy(src, dst, send_sem, recv_sem):
        return pltpu.make_async_remote_copy(
            src_ref=src,
            dst_ref=dst,
            send_sem=send_sem,
            recv_sem=recv_sem,
            device_id={"tp": other},
            device_id_type=MESH,
        )

    def norm_copy(c):
        rows = pl.ds(pl.multiple_of(me * half + c * BLOCK, BLOCK), BLOCK)
        return partner_copy(normed.at[rows], normed.at[rows], norm_send.at[c], norm_recv.at[c])

    outw_copies = [
        partner_copy(
            out_conv.at[:, pl.ds(c * piece, piece)],
            out_c.at[c, pl.ds(width, width)],
            outw_send.at[c],
            outw_recv.at[c],
        )
        for c in range(chunks)
    ] + [
        partner_copy(
            out_memory, out_m.at[pl.ds(width, width)], outw_send.at[chunks], outw_recv.at[chunks]
        )
    ]

    smalls[0].start()
    for c in tok_copies:
        c.start()
    for c in smalls[1:]:
        c.start()

    smalls[0].wait()
    w_copies[0].start()
    for j in range(norm_gain.shape[0]):
        gain_row[:, j * BLOCK : (j + 1) * BLOCK] = gain_in[j : j + 1].astype(F32)

    def normalize(c):
        for part in range(BLOCK // NORM_ROWS):
            start = c * BLOCK + part * NORM_ROWS
            x = tok[pl.ds(start, NORM_ROWS), :].astype(F32)
            scale = lax.rsqrt(jnp.mean(x * x, axis=-1, keepdims=True) + EPSILON)
            y = (x * scale) * gain_row[...]
            normed[pl.ds(pl.multiple_of(me * half + start, NORM_ROWS), NORM_ROWS), :] = y.astype(
                BF16
            )

    def gate_dot(c):
        rows = pl.ds(pl.multiple_of(me * half + c * BLOCK, BLOCK), BLOCK)
        gate_pre[rows, :] = jnp.dot(
            normed[rows, :], gate_w[...], preferred_element_type=F32
        )

    first_weights = 3
    smalls[1].wait()
    smalls[2].wait()
    gates = jnp.concatenate(
        [
            fgate_in[...],
            igate_in[...],
            jnp.zeros((BLOCK - 2 * PAD, igate_in.shape[1]), BF16),
        ],
        axis=0,
    )
    gate_w[...] = jnp.transpose(gates)
    for c in range(n_half):
        tok_copies[c].wait()
        if c + 1 < first_weights:
            w_copies[c + 1].start()
        if c > 0:
            gate_dot(c - 1)
        normalize(c)
        if c == 0:
            pl.semaphore_wait(barrier, jnp.where(place > 0, 2, 1))

            @pl.when(place > 0)
            def _():
                pl.semaphore_signal(
                    ready, inc=1, device_id={"sp": place - 1}, device_id_type=MESH
                )
        norm_copy(c).start()
    for c in w_copies[first_weights:]:
        c.start()

    for c in smalls[3:]:
        c.wait()
    head_rows[...] = head_in[...].astype(F32)

    @pl.when(place == 0)
    def _():
        for h in range(heads):
            carry[0, h] = init_memory[h].astype(BF16)
        carry_log[0] = jnp.zeros((PAD, BLOCK), F32)

    row_i = lax.broadcasted_iota(jnp.int32, (BLOCK, BLOCK), 0)
    col_i = lax.broadcasted_iota(jnp.int32, (BLOCK, BLOCK), 1)
    upper = jnp.where(row_i <= col_i, 1.0, 0.0).astype(F32)
    causal = col_i <= row_i

    first_head = me * heads
    to_front = lax.rem(PAD - first_head, PAD)
    lane_head = lax.broadcasted_iota(jnp.int32, (PAD, BLOCK), 0)
    bias_f = jnp.zeros((PAD, BLOCK), F32)
    bias_i = jnp.zeros((PAD, BLOCK), F32)
    for h in range(heads):
        bias_i = jnp.where(lane_head == h, bias_in[0, first_head + h], bias_i)
        bias_f = jnp.where(lane_head == h, bias_in[1, first_head + h], bias_f)
    no_head = jnp.zeros((PAD - heads, BLOCK), F32)

    def dot(a, b):
        return jnp.dot(a, b, preferred_element_type=F32)

    def project(target, slot, index, part, parts=PARTS):
        size = half // parts
        rows = rows_of(index * parts + part, size)
        target[rows, :] = dot(normed[rows, :], weights[slot]).astype(BF16)

    def gate_sums(index):
        forget_rows, in_rows = [], []
        for j in range(n_half):
            span = rows_of(index * n_half + j, BLOCK)
            pre = jnp.transpose(gate_pre[span, :])
            v = pltpu.roll(pre[0:PAD], to_front, 0) + bias_f
            log_forget = jnp.minimum(v, 0.0) - jnp.log1p(jnp.exp(-jnp.abs(v)))
            forget_rows.append(log_forget + jnp.concatenate([extra[:, span], no_head], axis=0))
            in_rows.append(pltpu.roll(pre[PAD : 2 * PAD], to_front, 0) + bias_i)
        all_cumulative = jnp.dot(
            jnp.concatenate(forget_rows, axis=0),
            upper,
            precision=lax.Precision.HIGHEST,
            preferred_element_type=F32,
        )
        return all_cumulative, jnp.concatenate(in_rows, axis=0)

    def gate_logs(index, all_cumulative, all_in):
        all_total = jnp.broadcast_to(all_cumulative[:, BLOCK - 1 : BLOCK], all_in.shape)
        exponent = all_total - all_cumulative + all_in
        all_peak = jnp.broadcast_to(jnp.max(exponent, axis=1, keepdims=True), all_in.shape)
        key_weight = jnp.exp(exponent - all_peak) * key_factor
        filler = jnp.zeros((BLOCK - 2 * PAD, BLOCK), F32)
        for j in range(n_half):
            b = index * n_half + j
            span = slice(j * PAD, (j + 1) * PAD)
            row_log[b, 0:PAD] = all_cumulative[span]
            row_log[b, PAD : 2 * PAD] = all_in[span]
            block_sum[b] = all_total[span]
            block_peak[b] = all_peak[span]
            col_log[b] = jnp.transpose(
                jnp.concatenate([all_cumulative[span], key_weight[span], filler], axis=0)
            )

    def block_terms(index):
        terms = []
        for h in range(heads):
            for j in range(n_half):
                b = index * n_half + j
                rows = rows_of(b, BLOCK)
                k = k_rows[rows, head_cols(h)].astype(F32)
                wk = (col_log[b, :, PAD + h : PAD + h + 1] * k).astype(BF16)
                terms.append(
                    lax.dot_general(
                        wk,
                        v_rows[rows, head_cols(h)],
                        (((0,), (0,)), ((), ())),
                        preferred_element_type=F32,
                    )
                )
        return terms

    def half_state(index, terms):
        log = jnp.full((PAD, BLOCK), LOWEST_LOG, F32)
        total = jnp.zeros((PAD, BLOCK), F32)
        filler = jnp.zeros((BLOCK - PAD, BLOCK), F32)
        keeps, adds = [], []
        for j in range(n_half):
            b = index * n_half + j
            prefix_cols[b] = jnp.transpose(jnp.concatenate([log, filler], axis=0))
            total_cols[b] = jnp.transpose(jnp.concatenate([total, filler], axis=0))
            now, peak = block_sum[b], block_peak[b]
            merged = jnp.maximum(now + log, peak)
            keeps.append(jnp.exp(now + log - merged))
            adds.append(jnp.exp(peak - merged))
            log = merged
            total = total + now
        half_log[index] = log
        half_total[index] = total
        for h in range(heads):
            state = jnp.zeros((dh, dh), F32)
            for j in range(n_half):
                prefix[index * n_half + j, h] = state.astype(BF16)
                state = (
                    keeps[j][h : h + 1] * state + adds[j][h : h + 1] * terms[h * n_half + j]
                )
            half_sum[index, h] = state

    def keys(index):
        for p in range(PARTS):
            project(k_rows, KEY, index, p)

    def values_queries(index):
        project(v_rows, VALUE, index, 0)
        sums = gate_sums(index)
        project(v_rows, VALUE, index, 1)
        gate_logs(index, *sums)
        project(q_rows, QUERY, index, 0)
        terms = block_terms(index)
        project(q_rows, QUERY, index, 1)
        half_state(index, terms)

    once = jnp.minimum(place + 1, 1)

    def region(body):
        pl.loop(0, once)(lambda _: body())

    w_copies[KEY].wait()
    @region
    def _():
        gate_dot(n_half - 1)
        keys(me)

    w_copies[VALUE].wait()
    w_copies[QUERY].wait()
    for c in out_copies:
        c.start()
    for c in outw_copies:
        c.start()
    @region
    def _():
        values_queries(me)

    for c in range(n_half):
        norm_copy(c).wait_recv()
    @region
    def _():
        other_rows = rows_of(other, half)
        gate_pre[other_rows, :] = dot(normed[other_rows, :], gate_w[...])
        keys(other)
        values_queries(other)

    for c in w_copies[GATE_IN:]:
        c.wait()

    def state_copies(k):
        span = pl.ds(k * group, group)
        pairs = [(send_memory.at[span], carry.at[0, span], k)]
        if k == 0:
            pairs.append((send_log, carry_log.at[0], BATCHES))
        return [
            pltpu.make_async_remote_copy(
                src_ref=src,
                dst_ref=dst,
                send_sem=state_send.at[s],
                recv_sem=state_recv.at[s],
                device_id={"sp": lax.rem(place + 1, n_sp)},
                device_id_type=MESH,
            )
            for src, dst, s in pairs
        ]

    def relay(k):
        @pl.when(place > 0)
        def _():
            for c in state_copies(k):
                c.wait_recv()

        if k == 0:
            log = carry_log[0]
            for i in range(2):
                now, peak = half_total[i], half_log[i]
                merged = jnp.maximum(now + log, peak)
                relay_rows[2 * i] = jnp.exp(now + log - merged)
                relay_rows[2 * i + 1] = jnp.exp(peak - merged)
                filler = jnp.zeros((BLOCK - PAD, BLOCK), F32)
                carry_cols[i] = jnp.transpose(jnp.concatenate([log, filler], axis=0))
                log = merged
            send_log[...] = log
        for h in range(k * group, (k + 1) * group):
            state = carry[0, h].astype(F32)
            for i in range(2):
                keep = relay_rows[2 * i, h : h + 1]
                add = relay_rows[2 * i + 1, h : h + 1]
                state = keep * state + add * half_sum[i, h]
                if i == 0:
                    carry[1, h] = state.astype(BF16)
            send_memory[h] = state.astype(BF16)

        @pl.when(place + 1 < n_sp)
        def _():
            for c in state_copies(k):
                c.start()

    n_main = 2 * n_half

    def relays(g):
        for k in range(BATCHES):
            due = jnp.where(place == 1, 2 + 2 * k, jnp.where(place == 2, 5 + k, n_main))
            due = jnp.where(place == 0, 0, due)

            @pl.when(due == g)
            def _(k=k):
                relay(k)

    def read_scores(b):
        rows = rows_of(b, BLOCK)
        return [
            lax.dot_general(
                q_rows[rows, head_cols(h)],
                k_rows[rows, head_cols(h)],
                (((1,), (1,)), ((), ())),
                preferred_element_type=F32,
            )
            for h in range(heads)
        ]

    def read_values(b, scores, tops, head_range):
        rows = rows_of(b, BLOCK)
        columns = col_log[b]
        carried_all = columns + prefix_cols[b]
        for h in head_range:
            pair = (columns[:, h : h + 1] - row_log[b, h : h + 1]) + row_log[
                b, PAD + h : PAD + h + 1
            ]
            pair = jnp.where(causal, pair, -jnp.inf)
            carried_log = carried_all[:, h : h + 1]
            top = jnp.maximum(carried_log, jnp.max(pair, axis=1, keepdims=True))
            weighted = (jnp.exp(pair - top) * (scores[h] * key_factor)).astype(BF16)
            q = q_rows[rows, head_cols(h)].astype(F32)
            carried = (jnp.exp(carried_log - top) * q).astype(BF16)
            local_out[rows, head_cols(h)] = dot(
                jnp.concatenate([weighted, carried], axis=1),
                jnp.concatenate([v_rows[rows, head_cols(h)], prefix[b, h]], axis=0),
            )
            tops = jnp.where(col_i == h, top, tops)
        return tops

    no_tops = jnp.zeros((BLOCK, BLOCK), F32)

    def unit(target, slot, index, reads, extras):
        scores = [read_scores(b) for b in reads]
        parts = max(len(extras), PARTS)
        tops = [no_tops] * len(reads)
        share = heads // PARTS
        for p in range(parts):
            project(target, slot, index, p, parts)
            if p < PARTS:
                for i, b in enumerate(reads):
                    tops[i] = read_values(
                        b, scores[i], tops[i], range(p * share, (p + 1) * share)
                    )
            if p < len(extras):
                extras[p]()
        for i, b in enumerate(reads):
            local_top[b] = tops[i]

    taps_cols = pl.ds(pl.multiple_of(me * width, width), width)
    taps = conv_taps[:, taps_cols].astype(F32)
    tap_count = conv_taps.shape[0]

    def product(rows, cols):
        return conv_pair[0, rows, cols].astype(F32) * conv_pair[1, rows, cols].astype(F32)

    def products(b):
        target = pl.ds(pl.multiple_of(RIM + b * BLOCK, RIM), BLOCK)
        for h in range(heads):
            conv_rows[h, target, :] = product(rows_of(b, BLOCK), head_cols(h))

    def convolve(b, slot, j):
        for h in range(heads):
            cols = head_cols(h)
            mixed = None
            for t in range(tap_count):
                x = conv_rows[h, pl.ds(b * BLOCK + (RIM - tap_count + 1 + t), BLOCK), :]
                y = x * taps[t : t + 1, cols]
                mixed = y if mixed is None else mixed + y
            mix_conv[slot, pl.ds(j * BLOCK, BLOCK), cols] = (
                go_rows[rows_of(b, BLOCK), cols].astype(F32) * mixed
            ).astype(BF16)

    split = n_main // 2

    late_reads = 2
    early_reads = nblocks - late_reads
    per_turn = early_reads // 2
    gi_rows, ci_rows = conv_pair.at[0], conv_pair.at[1]

    @pl.when(place + 1 < n_sp)
    def _():
        pl.semaphore_wait(ready, 1)

    @pl.loop(0, 2)
    def _(turn):
        relays(2 * turn)
        first = turn * per_turn
        cut = (per_turn + 1) // 2
        unit(gi_rows, GATE_IN, turn, [first + i for i in range(cut)], ())
        unit(ci_rows, CONV_IN, turn, [first + i for i in range(cut, per_turn)], ())

    for h in range(heads):
        rim_out[h] = product(pl.ds(total_rows - 2 * RIM, 2 * RIM), head_cols(h))[RIM:]
    rim_copy = pltpu.make_async_remote_copy(
        src_ref=rim_out,
        dst_ref=rim,
        send_sem=rim_sem.at[0],
        recv_sem=rim_sem.at[1],
        device_id={"sp": lax.rem(place + 1, n_sp)},
        device_id_type=MESH,
    )

    @pl.when(place + 1 < n_sp)
    def _():
        rim_copy.start()

    @pl.loop(split, split + 2)
    def _(g):
        relays(g)
        index = g - split
        unit(
            go_rows,
            GATE_OUT,
            index,
            [early_reads + index],
            [functools.partial(products, index * n_half + j) for j in range(n_half)],
        )

    @pl.when(place > 0)
    def _():
        rim_copy.wait_recv()
        conv_rows[:, 0:RIM, :] = rim[...]

    @pl.when(place == 0)
    def _():
        conv_rows[:, 0:RIM, :] = jnp.zeros((heads, RIM, dh), F32)

    conv_copy = partner_copy(
        mix_conv.at[1, :, pl.ds(0, width)],
        mix_conv.at[0, :, pl.ds(width, width)],
        conv_sem.at[0],
        conv_sem.at[1],
    )

    @pl.loop(split + 2, n_main)
    def _(g):
        relays(g)
        turn = g - (split + 2)
        side = jnp.where(turn == 0, other, me)
        unit(
            og_rows,
            OUT_GATE,
            turn,
            (),
            [
                functools.partial(convolve, side * n_half + j, 1 - turn, j)
                for j in range(n_half)
            ],
        )

        @pl.when(turn == 0)
        def _():
            conv_copy.start()

    relays(n_main)
    for c in out_copies:
        c.wait()
    for c in outw_copies:
        c.wait_recv()

    def factors(side, j):
        b = side * n_half + j
        local = local_top[b]
        carried_all = col_log[b] + total_cols[b] + carry_cols[side]
        top = jnp.maximum(local, carried_all)
        return jnp.exp(local - top), jnp.exp(carried_all - top)

    def finish_heads(side, slot, j, group, carried, local_factor, carried_factor):
        rows = rows_of(side * n_half + j, BLOCK)
        outs = [
            carried_factor[:, h : h + 1] * c
            + local_factor[:, h : h + 1] * local_out[rows, head_cols(h)]
            for h, c in zip(group, carried)
        ]
        means = [jnp.mean(out * out, axis=1, keepdims=True) for out in outs]
        gates = [
            head_rows[pl.ds(first_head + h, 1), :]
            * jax.nn.sigmoid(og_rows[rows, head_cols(h)].astype(F32))
            for h in group
        ]
        for h, out, mean, gate in zip(group, outs, means, gates):
            mix_memory[slot, rows_of(j, BLOCK), head_cols(h)] = (
                out * lax.rsqrt(mean + EPSILON) * gate
            ).astype(BF16)

    def memory_copy(j):
        rows = rows_of(j, BLOCK)
        return partner_copy(
            mix_memory.at[1, rows, pl.ds(0, width)],
            mix_memory.at[0, rows, pl.ds(width, width)],
            mem_send.at[j],
            mem_recv.at[j],
        )

    @pl.loop(0, 2)
    def _(turn):
        @pl.when(turn == 1)
        def _():
            conv_copy.wait_recv()
        side = jnp.where(turn == 0, other, me)
        share = heads // 2
        part_cols = rows_of(turn, width)
        in_chunks = chunks // 2
        for j in range(n_half):
            b_rows = rows_of(side * n_half + j, BLOCK)
            rows = slice(j * BLOCK, (j + 1) * BLOCK)
            mixed = factors(side, j)
            for i in range(2):
                group = range(i * share, (i + 1) * share)
                carried = [dot(q_rows[b_rows, head_cols(h)], carry[side, h]) for h in group]
                for c in range(i * in_chunks, (i + 1) * in_chunks):
                    acc[turn, rows, c * piece : (c + 1) * piece] = dot(
                        mix_conv[0, rows, part_cols], out_c[c, part_cols, :]
                    )
                finish_heads(side, 1 - turn, j, group, carried, *mixed)

        @pl.when(turn == 0)
        def _():
            for j in range(n_half):
                memory_copy(j).start()

    @region
    def _():
        acc[0] = acc[0] + acc[1] + dot(mix_memory[0, :, 0:width], out_m[0:width, :])

    for j in range(n_half):
        memory_copy(j).wait_recv()

    @region
    def _():
        layer_out[...] = (
            acc[0] + dot(mix_memory[0, :, width:], out_m[pl.ds(width, width), :])
        ).astype(BF16)

    for c in range(n_half):
        norm_copy(c).wait_send()
    for c in outw_copies:
        c.wait_send()
    conv_copy.wait_send()
    for j in range(n_half):
        memory_copy(j).wait_send()

    @pl.when(place + 1 < n_sp)
    def _():
        rim_copy.wait_send()
        for k in range(BATCHES):
            for c in state_copies(k):
                c.wait_send()


def local(
    tokens,
    norm_gain,
    w_query,
    w_key,
    w_value,
    w_outgate,
    w_gatein,
    w_gateout,
    w_convin,
    w_igate,
    w_fgate,
    input_bias,
    forget_bias,
    forget_extra,
    init_memory,
    head_gain,
    conv_taps,
    out_memory,
    out_conv,
):
    heads, dh = init_memory.shape[1], init_memory.shape[2]
    half, features = tokens.shape[1], tokens.shape[2]
    rows = forget_extra.shape[1]
    width = w_query.shape[1]
    nblocks = rows // BLOCK
    n_half = half // BLOCK
    all_heads = w_igate.shape[1]
    n_sp = lax.axis_size("sp")
    hbm = pl.BlockSpec(memory_space=pl.ANY)
    dma = pltpu.SemaphoreType.DMA
    out = pl.pallas_call(
        functools.partial(kernel, n_sp),
        name="layer",
        out_shape=pltpu.VMEM((half, features), BF16),
        in_specs=[hbm] * 19,
        out_specs=pl.BlockSpec(memory_space=pltpu.VMEM),
        scratch_shapes=[
            pltpu.VMEM((half, features), BF16),
            pltpu.VMEM((features // BLOCK, BLOCK), BF16),
            pltpu.VMEM((1, features), F32),
            pltpu.VMEM((all_heads, dh), BF16),
            pltpu.VMEM((all_heads, dh), F32),
            pltpu.VMEM((all_heads, features), BF16),
            pltpu.VMEM((all_heads, features), BF16),
            pltpu.VMEM((features, BLOCK), BF16),
            pltpu.SMEM((2, all_heads), F32),
            pltpu.VMEM((heads, rows), F32),
            pltpu.VMEM((heads, dh, dh), F32),
            pltpu.VMEM(conv_taps.shape, BF16),
            pltpu.VMEM((rows, features), BF16),
            pltpu.VMEM((7, features, width), BF16),
            pltpu.VMEM((2 * width, features), BF16),
            pltpu.VMEM((features // width, 2 * width, width), BF16),
            pltpu.VMEM((rows, width), BF16),
            pltpu.VMEM((rows, width), BF16),
            pltpu.VMEM((rows, width), BF16),
            pltpu.VMEM((2, rows, width), BF16),
            pltpu.VMEM((rows, width), BF16),
            pltpu.VMEM((rows, width), BF16),
            pltpu.VMEM((rows, BLOCK), F32),
            pltpu.VMEM((nblocks, 2 * PAD, BLOCK), F32),
            pltpu.VMEM((nblocks, BLOCK, BLOCK), F32),
            pltpu.VMEM((nblocks, PAD, BLOCK), F32),
            pltpu.VMEM((nblocks, PAD, BLOCK), F32),
            pltpu.VMEM((nblocks, heads, dh, dh), BF16),
            pltpu.VMEM((nblocks, BLOCK, BLOCK), F32),
            pltpu.VMEM((nblocks, BLOCK, BLOCK), F32),
            pltpu.VMEM((2, heads, dh, dh), F32),
            pltpu.VMEM((2, PAD, BLOCK), F32),
            pltpu.VMEM((2, PAD, BLOCK), F32),
            pltpu.VMEM((4, PAD, BLOCK), F32),
            pltpu.VMEM((2, heads, dh, dh), BF16),
            pltpu.VMEM((2, PAD, BLOCK), F32),
            pltpu.VMEM((2, BLOCK, BLOCK), F32),
            pltpu.VMEM((heads, dh, dh), BF16),
            pltpu.VMEM((PAD, BLOCK), F32),
            pltpu.VMEM((rows, width), F32),
            pltpu.VMEM((nblocks, BLOCK, BLOCK), F32),
            pltpu.VMEM((heads, RIM + rows, dh), F32),
            pltpu.VMEM((heads, RIM, dh), F32),
            pltpu.VMEM((heads, RIM, dh), F32),
            pltpu.VMEM((2, half, 2 * width), BF16),
            pltpu.VMEM((2, half, 2 * width), BF16),
            pltpu.VMEM((2, half, features), F32),
            dma((n_half,)),
            dma((9,)),
            dma((8 + features // width,)),
            dma((n_half,)),
            dma((n_half,)),
            dma((1 + features // width,)),
            dma((1 + features // width,)),
            dma((BATCHES + 1,)),
            dma((BATCHES + 1,)),
            pltpu.SemaphoreType.REGULAR,
            dma((2,)),
            dma((2,)),
            dma((n_half,)),
            dma((n_half,)),
        ],
        compiler_params=pltpu.CompilerParams(
            collective_id=0, has_side_effects=True, vmem_limit_bytes=60 * 1024 * 1024
        ),
    )(
        tokens[0],
        norm_gain.reshape(-1, BLOCK),
        w_key,
        w_value,
        w_query,
        w_gatein,
        w_convin,
        w_gateout,
        w_outgate,
        jnp.transpose(w_igate),
        jnp.transpose(w_fgate),
        input_bias,
        forget_bias,
        jnp.transpose(forget_extra[0]),
        init_memory[0],
        head_gain.reshape(-1, dh),
        conv_taps,
        out_memory,
        out_conv,
    )
    return out[None]


def solution(mesh):
    return jax.shard_map(
        local,
        mesh=mesh,
        in_specs=(
            P("fs", ("sp", "tp"), None),
            P(),
            P(None, "tp"),
            P(None, "tp"),
            P(None, "tp"),
            P(None, "tp"),
            P(None, "tp"),
            P(None, "tp"),
            P(None, "tp"),
            P(),
            P(),
            P(),
            P(),
            P("fs", "sp", "tp"),
            P("fs", "tp", None, None),
            P(),
            P(),
            P("tp", None),
            P("tp", None),
        ),
        out_specs=P("fs", ("sp", "tp"), None),
        check_vma=False,
    )
```

```python
import functools

import jax
import jax.numpy as jnp
from jax import lax
from jax.experimental import pallas as pl
from jax.experimental.pallas import tpu as pltpu
from jax.sharding import PartitionSpec as P

BLOCK = 128
EPSILON = 1e-06
LOWEST_LOG = -1e30
MESH = pl.DeviceIdType.MESH
F32 = jnp.float32
BF16 = jnp.bfloat16
PAD = 8
RIM = 8
NORM_ROWS = 64
BATCHES = 2
PARTS = 2

KEY, VALUE, QUERY, GATE_IN, CONV_IN, GATE_OUT, OUT_GATE = range(7)


def kernel(
    n_sp,
    tokens,
    norm_gain,
    w_key,
    w_value,
    w_query,
    w_gatein,
    w_convin,
    w_gateout,
    w_outgate,
    w_igate,
    w_fgate,
    input_bias,
    forget_bias,
    extra_in,
    init_in,
    head_gain,
    taps_in,
    out_memory,
    out_conv,
    layer_out,
    tok,
    gain_in,
    gain_row,
    head_in,
    head_rows,
    igate_in,
    fgate_in,
    gate_w,
    bias_in,
    extra,
    init_memory,
    conv_taps,
    normed,
    weights,
    out_m,
    out_c,
    k_rows,
    v_rows,
    q_rows,
    conv_pair,
    go_rows,
    og_rows,
    gate_pre,
    row_log,
    col_log,
    block_sum,
    block_peak,
    prefix,
    prefix_cols,
    total_cols,
    half_sum,
    half_log,
    half_total,
    relay_rows,
    carry,
    carry_log,
    carry_cols,
    send_memory,
    send_log,
    local_out,
    local_top,
    conv_rows,
    rim,
    rim_out,
    mix_conv,
    mix_memory,
    acc,
    token_sem,
    small_sem,
    weight_sem,
    norm_send,
    norm_recv,
    outw_send,
    outw_recv,
    state_send,
    state_recv,
    ready,
    rim_sem,
    conv_sem,
    mem_send,
    mem_recv,
):
    me = lax.axis_index("tp")
    other = 1 - me
    place = lax.axis_index("sp")
    half = tok.shape[0]
    total_rows = normed.shape[0]
    width = k_rows.shape[1]
    heads = init_memory.shape[0]
    dh = init_memory.shape[1]
    n_half = half // BLOCK
    nblocks = total_rows // BLOCK
    key_factor = dh ** (-0.5)
    out_width = layer_out.shape[1]
    group = heads // BATCHES
    chunks, piece = out_c.shape[0], out_c.shape[2]

    barrier = pltpu.get_barrier_semaphore()
    pl.semaphore_signal(barrier, inc=1, device_id={"tp": other}, device_id_type=MESH)

    @pl.when(place + 1 < n_sp)
    def _():
        pl.semaphore_signal(barrier, inc=1, device_id={"sp": place + 1}, device_id_type=MESH)

    def head_cols(h):
        return slice(h * dh, (h + 1) * dh)

    def rows_of(index, size):
        return pl.ds(pl.multiple_of(index * size, size), size)

    tok_copies = [
        pltpu.make_async_copy(
            tokens.at[pl.ds(c * BLOCK, BLOCK)], tok.at[pl.ds(c * BLOCK, BLOCK)], token_sem.at[c]
        )
        for c in range(n_half)
    ]
    smalls = [
        pltpu.make_async_copy(src, dst, small_sem.at[i])
        for i, (src, dst) in enumerate(
            (
                (norm_gain, gain_in),
                (w_igate, igate_in),
                (w_fgate, fgate_in),
                (input_bias, bias_in.at[0]),
                (forget_bias, bias_in.at[1]),
                (extra_in, extra),
                (init_in, init_memory),
                (head_gain, head_in),
                (taps_in, conv_taps),
            )
        )
    ]
    w_in = (w_key, w_value, w_query, w_gatein, w_convin, w_gateout, w_outgate)
    w_copies = [
        pltpu.make_async_copy(w, weights.at[s], weight_sem.at[s]) for s, w in enumerate(w_in)
    ]
    out_copies = [
        pltpu.make_async_copy(out_memory, out_m.at[pl.ds(0, width)], weight_sem.at[7]),
    ] + [
        pltpu.make_async_copy(
            out_conv.at[:, pl.ds(c * piece, piece)], out_c.at[c, pl.ds(0, width)], weight_sem.at[8 + c]
        )
        for c in range(chunks)
    ]

    def partner_copy(src, dst, send_sem, recv_sem):
        return pltpu.make_async_remote_copy(
            src_ref=src,
            dst_ref=dst,
            send_sem=send_sem,
            recv_sem=recv_sem,
            device_id={"tp": other},
            device_id_type=MESH,
        )

    def norm_copy(c):
        rows = pl.ds(pl.multiple_of(me * half + c * BLOCK, BLOCK), BLOCK)
        return partner_copy(normed.at[rows], normed.at[rows], norm_send.at[c], norm_recv.at[c])

    outw_copies = [
        partner_copy(
            out_conv.at[:, pl.ds(c * piece, piece)],
            out_c.at[c, pl.ds(width, width)],
            outw_send.at[c],
            outw_recv.at[c],
        )
        for c in range(chunks)
    ] + [
        partner_copy(
            out_memory, out_m.at[pl.ds(width, width)], outw_send.at[chunks], outw_recv.at[chunks]
        )
    ]

    smalls[0].start()
    for c in tok_copies:
        c.start()
    for c in smalls[1:]:
        c.start()

    smalls[0].wait()
    w_copies[0].start()
    for j in range(norm_gain.shape[0]):
        gain_row[:, j * BLOCK : (j + 1) * BLOCK] = gain_in[j : j + 1].astype(F32)

    def normalize(c):
        for part in range(BLOCK // NORM_ROWS):
            start = c * BLOCK + part * NORM_ROWS
            x = tok[pl.ds(start, NORM_ROWS), :].astype(F32)
            scale = lax.rsqrt(jnp.mean(x * x, axis=-1, keepdims=True) + EPSILON)
            y = (x * scale) * gain_row[...]
            normed[pl.ds(pl.multiple_of(me * half + start, NORM_ROWS), NORM_ROWS), :] = y.astype(
                BF16
            )

    def gate_dot(c):
        rows = pl.ds(pl.multiple_of(me * half + c * BLOCK, BLOCK), BLOCK)
        gate_pre[rows, :] = jnp.dot(
            normed[rows, :], gate_w[...], preferred_element_type=F32
        )

    first_weights = 3
    smalls[1].wait()
    smalls[2].wait()
    gates = jnp.concatenate(
        [
            fgate_in[...],
            igate_in[...],
            jnp.zeros((BLOCK - 2 * PAD, igate_in.shape[1]), BF16),
        ],
        axis=0,
    )
    gate_w[...] = jnp.transpose(gates)
    for c in range(n_half):
        tok_copies[c].wait()
        if c + 1 < first_weights:
            w_copies[c + 1].start()
        if c > 0:
            gate_dot(c - 1)
        normalize(c)
        if c == 0:
            pl.semaphore_wait(barrier, jnp.where(place > 0, 2, 1))

            @pl.when(place > 0)
            def _():
                pl.semaphore_signal(
                    ready, inc=1, device_id={"sp": place - 1}, device_id_type=MESH
                )
        norm_copy(c).start()
    for c in w_copies[first_weights:]:
        c.start()

    for c in smalls[3:]:
        c.wait()
    head_rows[...] = head_in[...].astype(F32)

    @pl.when(place == 0)
    def _():
        for h in range(heads):
            carry[0, h] = init_memory[h].astype(BF16)
        carry_log[0] = jnp.zeros((PAD, BLOCK), F32)

    row_i = lax.broadcasted_iota(jnp.int32, (BLOCK, BLOCK), 0)
    col_i = lax.broadcasted_iota(jnp.int32, (BLOCK, BLOCK), 1)
    upper = jnp.where(row_i <= col_i, 1.0, 0.0).astype(F32)
    causal = col_i <= row_i

    first_head = me * heads
    to_front = lax.rem(PAD - first_head, PAD)
    lane_head = lax.broadcasted_iota(jnp.int32, (PAD, BLOCK), 0)
    bias_f = jnp.zeros((PAD, BLOCK), F32)
    bias_i = jnp.zeros((PAD, BLOCK), F32)
    for h in range(heads):
        bias_i = jnp.where(lane_head == h, bias_in[0, first_head + h], bias_i)
        bias_f = jnp.where(lane_head == h, bias_in[1, first_head + h], bias_f)
    no_head = jnp.zeros((PAD - heads, BLOCK), F32)

    def dot(a, b):
        return jnp.dot(a, b, preferred_element_type=F32)

    def project(target, slot, index, part, parts=PARTS):
        size = half // parts
        rows = rows_of(index * parts + part, size)
        target[rows, :] = dot(normed[rows, :], weights[slot]).astype(BF16)

    def gate_sums(index):
        forget_rows, in_rows = [], []
        for j in range(n_half):
            span = rows_of(index * n_half + j, BLOCK)
            pre = jnp.transpose(gate_pre[span, :])
            v = pltpu.roll(pre[0:PAD], to_front, 0) + bias_f
            log_forget = jnp.minimum(v, 0.0) - jnp.log1p(jnp.exp(-jnp.abs(v)))
            forget_rows.append(log_forget + jnp.concatenate([extra[:, span], no_head], axis=0))
            in_rows.append(pltpu.roll(pre[PAD : 2 * PAD], to_front, 0) + bias_i)
        all_cumulative = jnp.dot(
            jnp.concatenate(forget_rows, axis=0),
            upper,
            precision=lax.Precision.HIGHEST,
            preferred_element_type=F32,
        )
        return all_cumulative, jnp.concatenate(in_rows, axis=0)

    def gate_logs(index, all_cumulative, all_in):
        all_total = jnp.broadcast_to(all_cumulative[:, BLOCK - 1 : BLOCK], all_in.shape)
        exponent = all_total - all_cumulative + all_in
        all_peak = jnp.broadcast_to(jnp.max(exponent, axis=1, keepdims=True), all_in.shape)
        key_weight = jnp.exp(exponent - all_peak) * key_factor
        filler = jnp.zeros((BLOCK - 2 * PAD, BLOCK), F32)
        for j in range(n_half):
            b = index * n_half + j
            span = slice(j * PAD, (j + 1) * PAD)
            row_log[b, 0:PAD] = all_cumulative[span]
            row_log[b, PAD : 2 * PAD] = all_in[span]
            block_sum[b] = all_total[span]
            block_peak[b] = all_peak[span]
            col_log[b] = jnp.transpose(
                jnp.concatenate([all_cumulative[span], key_weight[span], filler], axis=0)
            )

    def block_terms(index):
        terms = []
        for h in range(heads):
            for j in range(n_half):
                b = index * n_half + j
                rows = rows_of(b, BLOCK)
                k = k_rows[rows, head_cols(h)].astype(F32)
                wk = (col_log[b, :, PAD + h : PAD + h + 1] * k).astype(BF16)
                terms.append(
                    lax.dot_general(
                        wk,
                        v_rows[rows, head_cols(h)],
                        (((0,), (0,)), ((), ())),
                        preferred_element_type=F32,
                    )
                )
        return terms

    def half_state(index, terms):
        log = jnp.full((PAD, BLOCK), LOWEST_LOG, F32)
        total = jnp.zeros((PAD, BLOCK), F32)
        filler = jnp.zeros((BLOCK - PAD, BLOCK), F32)
        keeps, adds = [], []
        for j in range(n_half):
            b = index * n_half + j
            prefix_cols[b] = jnp.transpose(jnp.concatenate([log, filler], axis=0))
            total_cols[b] = jnp.transpose(jnp.concatenate([total, filler], axis=0))
            now, peak = block_sum[b], block_peak[b]
            merged = jnp.maximum(now + log, peak)
            keeps.append(jnp.exp(now + log - merged))
            adds.append(jnp.exp(peak - merged))
            log = merged
            total = total + now
        half_log[index] = log
        half_total[index] = total
        for h in range(heads):
            state = jnp.zeros((dh, dh), F32)
            for j in range(n_half):
                prefix[index * n_half + j, h] = state.astype(BF16)
                state = (
                    keeps[j][h : h + 1] * state + adds[j][h : h + 1] * terms[h * n_half + j]
                )
            half_sum[index, h] = state

    def keys(index):
        for p in range(PARTS):
            project(k_rows, KEY, index, p)

    def values_queries(index):
        project(v_rows, VALUE, index, 0)
        sums = gate_sums(index)
        project(v_rows, VALUE, index, 1)
        gate_logs(index, *sums)
        project(q_rows, QUERY, index, 0)
        terms = block_terms(index)
        project(q_rows, QUERY, index, 1)
        half_state(index, terms)

    once = jnp.minimum(place + 1, 1)

    def region(body):
        pl.loop(0, once)(lambda _: body())

    w_copies[KEY].wait()
    @region
    def _():
        gate_dot(n_half - 1)
        keys(me)

    w_copies[VALUE].wait()
    w_copies[QUERY].wait()
    for c in out_copies:
        c.start()
    for c in outw_copies:
        c.start()
    @region
    def _():
        values_queries(me)

    for c in range(n_half):
        norm_copy(c).wait_recv()
    @region
    def _():
        other_rows = rows_of(other, half)
        gate_pre[other_rows, :] = dot(normed[other_rows, :], gate_w[...])
        keys(other)
        values_queries(other)

    for c in w_copies[GATE_IN:]:
        c.wait()

    def state_copies(k):
        span = pl.ds(k * group, group)
        pairs = [(send_memory.at[span], carry.at[0, span], k)]
        if k == 0:
            pairs.append((send_log, carry_log.at[0], BATCHES))
        return [
            pltpu.make_async_remote_copy(
                src_ref=src,
                dst_ref=dst,
                send_sem=state_send.at[s],
                recv_sem=state_recv.at[s],
                device_id={"sp": lax.rem(place + 1, n_sp)},
                device_id_type=MESH,
            )
            for src, dst, s in pairs
        ]

    def relay(k):
        @pl.when(place > 0)
        def _():
            for c in state_copies(k):
                c.wait_recv()

        if k == 0:
            log = carry_log[0]
            for i in range(2):
                now, peak = half_total[i], half_log[i]
                merged = jnp.maximum(now + log, peak)
                relay_rows[2 * i] = jnp.exp(now + log - merged)
                relay_rows[2 * i + 1] = jnp.exp(peak - merged)
                filler = jnp.zeros((BLOCK - PAD, BLOCK), F32)
                carry_cols[i] = jnp.transpose(jnp.concatenate([log, filler], axis=0))
                log = merged
            send_log[...] = log
        for h in range(k * group, (k + 1) * group):
            state = carry[0, h].astype(F32)
            for i in range(2):
                keep = relay_rows[2 * i, h : h + 1]
                add = relay_rows[2 * i + 1, h : h + 1]
                state = keep * state + add * half_sum[i, h]
                if i == 0:
                    carry[1, h] = state.astype(BF16)
            send_memory[h] = state.astype(BF16)

        @pl.when(place + 1 < n_sp)
        def _():
            for c in state_copies(k):
                c.start()

    n_main = 2 * n_half

    def relays(g):
        for k in range(BATCHES):
            due = jnp.where(place == 1, 2 + 2 * k, jnp.where(place == 2, 5 + k, n_main))
            due = jnp.where(place == 0, 0, due)

            @pl.when(due == g)
            def _(k=k):
                relay(k)

    def read_scores(b):
        rows = rows_of(b, BLOCK)
        return [
            lax.dot_general(
                q_rows[rows, head_cols(h)],
                k_rows[rows, head_cols(h)],
                (((1,), (1,)), ((), ())),
                preferred_element_type=F32,
            )
            for h in range(heads)
        ]

    def read_values(b, scores, tops, head_range):
        rows = rows_of(b, BLOCK)
        columns = col_log[b]
        carried_all = columns + prefix_cols[b]
        for h in head_range:
            pair = (columns[:, h : h + 1] - row_log[b, h : h + 1]) + row_log[
                b, PAD + h : PAD + h + 1
            ]
            pair = jnp.where(causal, pair, -jnp.inf)
            carried_log = carried_all[:, h : h + 1]
            top = jnp.maximum(carried_log, jnp.max(pair, axis=1, keepdims=True))
            weighted = (jnp.exp(pair - top) * (scores[h] * key_factor)).astype(BF16)
            q = q_rows[rows, head_cols(h)].astype(F32)
            carried = (jnp.exp(carried_log - top) * q).astype(BF16)
            local_out[rows, head_cols(h)] = dot(
                jnp.concatenate([weighted, carried], axis=1),
                jnp.concatenate([v_rows[rows, head_cols(h)], prefix[b, h]], axis=0),
            )
            tops = jnp.where(col_i == h, top, tops)
        return tops

    no_tops = jnp.zeros((BLOCK, BLOCK), F32)

    def unit(target, slot, index, reads, extras):
        scores = [read_scores(b) for b in reads]
        parts = max(len(extras), PARTS)
        tops = [no_tops] * len(reads)
        share = heads // PARTS
        for p in range(parts):
            project(target, slot, index, p, parts)
            if p < PARTS:
                for i, b in enumerate(reads):
                    tops[i] = read_values(
                        b, scores[i], tops[i], range(p * share, (p + 1) * share)
                    )
            if p < len(extras):
                extras[p]()
        for i, b in enumerate(reads):
            local_top[b] = tops[i]

    taps_cols = pl.ds(pl.multiple_of(me * width, width), width)
    taps = conv_taps[:, taps_cols].astype(F32)
    tap_count = conv_taps.shape[0]

    def product(rows, cols):
        return conv_pair[0, rows, cols].astype(F32) * conv_pair[1, rows, cols].astype(F32)

    def products(b):
        target = pl.ds(pl.multiple_of(RIM + b * BLOCK, RIM), BLOCK)
        for h in range(heads):
            conv_rows[h, target, :] = product(rows_of(b, BLOCK), head_cols(h))

    def convolve(b, slot, j):
        for h in range(heads):
            cols = head_cols(h)
            mixed = None
            for t in range(tap_count):
                x = conv_rows[h, pl.ds(b * BLOCK + (RIM - tap_count + 1 + t), BLOCK), :]
                y = x * taps[t : t + 1, cols]
                mixed = y if mixed is None else mixed + y
            mix_conv[slot, pl.ds(j * BLOCK, BLOCK), cols] = (
                go_rows[rows_of(b, BLOCK), cols].astype(F32) * mixed
            ).astype(BF16)

    split = n_main // 2

    late_reads = 2
    early_reads = nblocks - late_reads
    per_turn = early_reads // 2
    gi_rows, ci_rows = conv_pair.at[0], conv_pair.at[1]

    @pl.when(place + 1 < n_sp)
    def _():
        pl.semaphore_wait(ready, 1)

    @pl.loop(0, 2)
    def _(turn):
        relays(2 * turn)
        first = turn * per_turn
        cut = (per_turn + 1) // 2
        unit(gi_rows, GATE_IN, turn, [first + i for i in range(cut)], ())
        unit(ci_rows, CONV_IN, turn, [first + i for i in range(cut, per_turn)], ())

    for h in range(heads):
        rim_out[h] = product(pl.ds(total_rows - 2 * RIM, 2 * RIM), head_cols(h))[RIM:]
    rim_copy = pltpu.make_async_remote_copy(
        src_ref=rim_out,
        dst_ref=rim,
        send_sem=rim_sem.at[0],
        recv_sem=rim_sem.at[1],
        device_id={"sp": lax.rem(place + 1, n_sp)},
        device_id_type=MESH,
    )

    @pl.when(place + 1 < n_sp)
    def _():
        rim_copy.start()

    @pl.loop(split, split + 2)
    def _(g):
        relays(g)
        index = g - split
        unit(
            go_rows,
            GATE_OUT,
            index,
            [early_reads + index],
            [functools.partial(products, index * n_half + j) for j in range(n_half)],
        )

    @pl.when(place > 0)
    def _():
        rim_copy.wait_recv()
        conv_rows[:, 0:RIM, :] = rim[...]

    @pl.when(place == 0)
    def _():
        conv_rows[:, 0:RIM, :] = jnp.zeros((heads, RIM, dh), F32)

    conv_copy = partner_copy(
        mix_conv.at[1, :, pl.ds(0, width)],
        mix_conv.at[0, :, pl.ds(width, width)],
        conv_sem.at[0],
        conv_sem.at[1],
    )

    relays(split + 2)

    @region
    def _():
        for turn, side in enumerate((other, me)):
            unit(
                og_rows,
                OUT_GATE,
                turn,
                (),
                [
                    functools.partial(convolve, side * n_half + j, 1 - turn, j)
                    for j in range(n_half)
                ],
            )
            if turn == 0:
                conv_copy.start()

    relays(n_main)
    for c in out_copies:
        c.wait()
    for c in outw_copies:
        c.wait_recv()

    def factors(side, j):
        b = side * n_half + j
        local = local_top[b]
        carried_all = col_log[b] + total_cols[b] + carry_cols[side]
        top = jnp.maximum(local, carried_all)
        return jnp.exp(local - top), jnp.exp(carried_all - top)

    def finish_heads(side, slot, j, group, carried, local_factor, carried_factor):
        rows = rows_of(side * n_half + j, BLOCK)
        outs = [
            carried_factor[:, h : h + 1] * c
            + local_factor[:, h : h + 1] * local_out[rows, head_cols(h)]
            for h, c in zip(group, carried)
        ]
        means = [jnp.mean(out * out, axis=1, keepdims=True) for out in outs]
        gates = [
            head_rows[pl.ds(first_head + h, 1), :]
            * jax.nn.sigmoid(og_rows[rows, head_cols(h)].astype(F32))
            for h in group
        ]
        for h, out, mean, gate in zip(group, outs, means, gates):
            mix_memory[slot, rows_of(j, BLOCK), head_cols(h)] = (
                out * lax.rsqrt(mean + EPSILON) * gate
            ).astype(BF16)

    def memory_copy(j):
        rows = rows_of(j, BLOCK)
        return partner_copy(
            mix_memory.at[1, rows, pl.ds(0, width)],
            mix_memory.at[0, rows, pl.ds(width, width)],
            mem_send.at[j],
            mem_recv.at[j],
        )

    @pl.loop(0, 2)
    def _(turn):
        @pl.when(turn == 1)
        def _():
            conv_copy.wait_recv()
        side = jnp.where(turn == 0, other, me)
        share = heads // 2
        part_cols = rows_of(turn, width)
        in_chunks = chunks // 2
        for j in range(n_half):
            b_rows = rows_of(side * n_half + j, BLOCK)
            rows = slice(j * BLOCK, (j + 1) * BLOCK)
            mixed = factors(side, j)
            for i in range(2):
                group = range(i * share, (i + 1) * share)
                carried = [dot(q_rows[b_rows, head_cols(h)], carry[side, h]) for h in group]
                for c in range(i * in_chunks, (i + 1) * in_chunks):
                    acc[turn, rows, c * piece : (c + 1) * piece] = dot(
                        mix_conv[0, rows, part_cols], out_c[c, part_cols, :]
                    )
                finish_heads(side, 1 - turn, j, group, carried, *mixed)

        @pl.when(turn == 0)
        def _():
            for j in range(n_half):
                memory_copy(j).start()

    @region
    def _():
        acc[0] = acc[0] + acc[1] + dot(mix_memory[0, :, 0:width], out_m[0:width, :])

    for j in range(n_half):
        memory_copy(j).wait_recv()

    @region
    def _():
        layer_out[...] = (
            acc[0] + dot(mix_memory[0, :, width:], out_m[pl.ds(width, width), :])
        ).astype(BF16)

    for c in range(n_half):
        norm_copy(c).wait_send()
    for c in outw_copies:
        c.wait_send()
    conv_copy.wait_send()
    for j in range(n_half):
        memory_copy(j).wait_send()

    @pl.when(place + 1 < n_sp)
    def _():
        rim_copy.wait_send()
        for k in range(BATCHES):
            for c in state_copies(k):
                c.wait_send()


def local(
    tokens,
    norm_gain,
    w_query,
    w_key,
    w_value,
    w_outgate,
    w_gatein,
    w_gateout,
    w_convin,
    w_igate,
    w_fgate,
    input_bias,
    forget_bias,
    forget_extra,
    init_memory,
    head_gain,
    conv_taps,
    out_memory,
    out_conv,
):
    heads, dh = init_memory.shape[1], init_memory.shape[2]
    half, features = tokens.shape[1], tokens.shape[2]
    rows = forget_extra.shape[1]
    width = w_query.shape[1]
    nblocks = rows // BLOCK
    n_half = half // BLOCK
    all_heads = w_igate.shape[1]
    n_sp = lax.axis_size("sp")
    hbm = pl.BlockSpec(memory_space=pl.ANY)
    dma = pltpu.SemaphoreType.DMA
    out = pl.pallas_call(
        functools.partial(kernel, n_sp),
        name="layer",
        out_shape=pltpu.VMEM((half, features), BF16),
        in_specs=[hbm] * 19,
        out_specs=pl.BlockSpec(memory_space=pltpu.VMEM),
        scratch_shapes=[
            pltpu.VMEM((half, features), BF16),
            pltpu.VMEM((features // BLOCK, BLOCK), BF16),
            pltpu.VMEM((1, features), F32),
            pltpu.VMEM((all_heads, dh), BF16),
            pltpu.VMEM((all_heads, dh), F32),
            pltpu.VMEM((all_heads, features), BF16),
            pltpu.VMEM((all_heads, features), BF16),
            pltpu.VMEM((features, BLOCK), BF16),
            pltpu.SMEM((2, all_heads), F32),
            pltpu.VMEM((heads, rows), F32),
            pltpu.VMEM((heads, dh, dh), F32),
            pltpu.VMEM(conv_taps.shape, BF16),
            pltpu.VMEM((rows, features), BF16),
            pltpu.VMEM((7, features, width), BF16),
            pltpu.VMEM((2 * width, features), BF16),
            pltpu.VMEM((features // width, 2 * width, width), BF16),
            pltpu.VMEM((rows, width), BF16),
            pltpu.VMEM((rows, width), BF16),
            pltpu.VMEM((rows, width), BF16),
            pltpu.VMEM((2, rows, width), BF16),
            pltpu.VMEM((rows, width), BF16),
            pltpu.VMEM((rows, width), BF16),
            pltpu.VMEM((rows, BLOCK), F32),
            pltpu.VMEM((nblocks, 2 * PAD, BLOCK), F32),
            pltpu.VMEM((nblocks, BLOCK, BLOCK), F32),
            pltpu.VMEM((nblocks, PAD, BLOCK), F32),
            pltpu.VMEM((nblocks, PAD, BLOCK), F32),
            pltpu.VMEM((nblocks, heads, dh, dh), BF16),
            pltpu.VMEM((nblocks, BLOCK, BLOCK), F32),
            pltpu.VMEM((nblocks, BLOCK, BLOCK), F32),
            pltpu.VMEM((2, heads, dh, dh), F32),
            pltpu.VMEM((2, PAD, BLOCK), F32),
            pltpu.VMEM((2, PAD, BLOCK), F32),
            pltpu.VMEM((4, PAD, BLOCK), F32),
            pltpu.VMEM((2, heads, dh, dh), BF16),
            pltpu.VMEM((2, PAD, BLOCK), F32),
            pltpu.VMEM((2, BLOCK, BLOCK), F32),
            pltpu.VMEM((heads, dh, dh), BF16),
            pltpu.VMEM((PAD, BLOCK), F32),
            pltpu.VMEM((rows, width), F32),
            pltpu.VMEM((nblocks, BLOCK, BLOCK), F32),
            pltpu.VMEM((heads, RIM + rows, dh), F32),
            pltpu.VMEM((heads, RIM, dh), F32),
            pltpu.VMEM((heads, RIM, dh), F32),
            pltpu.VMEM((2, half, 2 * width), BF16),
            pltpu.VMEM((2, half, 2 * width), BF16),
            pltpu.VMEM((2, half, features), F32),
            dma((n_half,)),
            dma((9,)),
            dma((8 + features // width,)),
            dma((n_half,)),
            dma((n_half,)),
            dma((1 + features // width,)),
            dma((1 + features // width,)),
            dma((BATCHES + 1,)),
            dma((BATCHES + 1,)),
            pltpu.SemaphoreType.REGULAR,
            dma((2,)),
            dma((2,)),
            dma((n_half,)),
            dma((n_half,)),
        ],
        compiler_params=pltpu.CompilerParams(
            collective_id=0, has_side_effects=True, vmem_limit_bytes=60 * 1024 * 1024
        ),
    )(
        tokens[0],
        norm_gain.reshape(-1, BLOCK),
        w_key,
        w_value,
        w_query,
        w_gatein,
        w_convin,
        w_gateout,
        w_outgate,
        jnp.transpose(w_igate),
        jnp.transpose(w_fgate),
        input_bias,
        forget_bias,
        jnp.transpose(forget_extra[0]),
        init_memory[0],
        head_gain.reshape(-1, dh),
        conv_taps,
        out_memory,
        out_conv,
    )
    return out[None]


def solution(mesh):
    return jax.shard_map(
        local,
        mesh=mesh,
        in_specs=(
            P("fs", ("sp", "tp"), None),
            P(),
            P(None, "tp"),
            P(None, "tp"),
            P(None, "tp"),
            P(None, "tp"),
            P(None, "tp"),
            P(None, "tp"),
            P(None, "tp"),
            P(),
            P(),
            P(),
            P(),
            P("fs", "sp", "tp"),
            P("fs", "tp", None, None),
            P(),
            P(),
            P("tp", None),
            P("tp", None),
        ),
        out_specs=P("fs", ("sp", "tp"), None),
        check_vma=False,
    )
```
